512 devices in a mesh: ep: 32 (over z, x), tp: 16 (over y, core).
Axes of the slice: x: 4, y: 8, z: 8, core: 2. Of those that a mesh axis runs over, the one named last changes fastest.
Arguments:
- queries: bfloat16 [24576, 1024], P('ep', 'tp'), may hold values from -6.5 to 6.5
- keys: bfloat16 [24576, 1024], P('ep', 'tp'), may hold values from -6.5 to 6.5
- values: bfloat16 [24576, 1024], P('ep', 'tp'), may hold values from -6 to 6
- cum_gate: float32 [24576, 16], P('ep', 'tp'), may hold values from -3074 to 0, as said below
- head_gain: float32 [1024], P('tp'), may hold values from 0.1 to 1.9
- moe_in: bfloat16 [4096, 2048], P('ep'), may hold values from -6 to 6
- ffn_gain: float32 [2048], replicated, may hold values from 0.1 to 1.9
- routes: int32 [4096, 4], P('ep'), may hold values from 0 to 127, all different within a row; in each aligned block of 128 rows (0 to 127, 128 to 255, ...) at most 6 rows name the same one
- route_weight: float32 [4096, 4], P('ep'), may hold values from 0.2 to 1.2
- expert_gate: bfloat16 [128, 1024, 2048], P('ep', 'tp'), may hold values from -0.125 to 0.125
- expert_up: bfloat16 [128, 1024, 2048], P('ep', 'tp'), may hold values from -0.125 to 0.125
- expert_down: bfloat16 [128, 1024, 2048], P('ep', 'tp'), may hold values from -0.25 to 0.25
- shared_gate: bfloat16 [512, 2048], P('tp'), may hold values from -0.125 to 0.125
- shared_up: bfloat16 [512, 2048], P('tp'), may hold values from -0.125 to 0.125
- shared_down: bfloat16 [512, 2048], P('tp'), may hold values from -0.375 to 0.375
Outputs:
- mixed: bfloat16 [24576, 1024], P('ep', 'tp')
- expert_out: bfloat16 [4096, 2048], P('ep', 'tp')
The draws below stay inside these ranges and needn't reach their ends.
Inputs may be any that keep to these rules, and one draw needn't show every extreme that they name: `routes`: in each aligned block of 128 rows (the tokens of one index of ep) no expert is named by more than 6 rows, a bound that some block reaches; a row names 4 different experts. Each head's cum_gate never rises from one position to the next.
All inputs are finite; a program needn't handle non-finite values.
Results may differ from the reference program's by a relative error of at most 0.019.
Values may be sent and summed in bfloat16 or wider, within the bound.
No kernel may reach another device: no remote copies, remote signals or barrier semaphores. Data moves between devices by JAX's collectives and lax.ppermute only.
A program may use at most 128 MiB of HBM per device.

```python
import math
import jax
import jax.numpy as jnp
import numpy as np
from jax import lax

D = 2048
HEADS = 16
HEAD = 64
FF_E = 1024
SHARED = 512
TOP = 4
ROWS = 768
MROWS = 128
SEQ = 24576
QW = 1024
MTOK = 4096
EXPERTS = 128
CAP = 6
N_EP = 32
N_TP = 16


def plant_pairs(key):
    base = jax.random.fold_in(key, 7)
    streams = jax.random.split(base, 2)
    query_rows = jnp.clip(jax.random.normal(streams[0], (SEQ, QW), jnp.float32), -6.0, 6.0)
    key_rows = jnp.clip(jax.random.normal(streams[1], (SEQ, QW), jnp.float32), -6.0, 6.0)
    return (query_rows, key_rows)


def draw_queries(key, part):
    return plant_pairs(key)[0].astype(jnp.bfloat16)


def draw_keys(key, part):
    return plant_pairs(key)[1].astype(jnp.bfloat16)


def draw_cum_gate(key, part):
    base = jax.random.fold_in(key, 11)
    streams = jax.random.split(base, 6)
    order = jax.random.permutation(streams[0], HEADS)
    slow_heads = order >= HEADS // 2
    fast_rate = jnp.exp(jax.random.uniform(streams[1], (HEADS,), jnp.float32, math.log(1.0 / 100.0), math.log(1.0 / 30.0)))
    fading_speed = jnp.where(slow_heads, 0.6 / SEQ, fast_rate)
    extent_coefficient = jnp.exp(jax.random.uniform(streams[2], (SEQ // ROWS,), jnp.float32, math.log(0.5), math.log(2.0)))
    extent_coefficient = jnp.repeat(extent_coefficient, ROWS)
    approximate_guess = jax.random.uniform(streams[3], (SEQ, HEADS), jnp.float32, 0.3, 1.7)
    spots = jax.random.randint(streams[4], (3,), 0, SEQ)
    discarded_items = jax.random.uniform(streams[5], (3, HEADS), jnp.float32, 0.22, 0.5)
    agreement_tally = (jnp.arange(SEQ)[:, None] == spots[None, :]).astype(jnp.float32)
    spike_occurrences = jnp.dot(agreement_tally, discarded_items)
    objective_list = fading_speed[None, :] * approximate_guess * extent_coefficient[:, None] + spike_occurrences
    return -jnp.cumsum(objective_list, axis=0)


def spiked(drawn, stream_key, source, target, parts, factor):
    def block_of(position):
        return (jnp.arange(drawn.shape[position]) // (drawn.shape[position] // parts)).reshape((-1,) + (1,) * (drawn.ndim - 1 - position))

    first = jax.random.permutation(stream_key, parts)[block_of(target)]
    second = (block_of(target) + parts // 2) % parts
    return jnp.where((block_of(source) == first) | (block_of(source) == second), factor * drawn, drawn)


def levels(stream_key, extent, cuts, smallest, top_value):
    level, own = 1.0, jax.random.fold_in(stream_key, 6)
    for axis_at, shards_of in cuts:
        draws = jnp.exp(jax.random.uniform(jax.random.fold_in(own, axis_at), (shards_of,), jnp.float32, smallest / len(cuts), top_value / len(cuts)))
        level = level * jnp.repeat(draws, extent[axis_at] // shards_of).reshape([-1 if axis == axis_at else 1 for axis in range(len(extent))])
    return level


def assign_block(own_key, own, number, rows, number_of, top, bound, skew):
    sequence = jax.random.permutation(own_key, number_of)
    heavy_load, common = load_shares(number_of, rows * top, bound, skew, True), load_shares(number_of, rows * top, bound, skew, False)
    places = jnp.arange(number_of)

    def named(tallies, offset_by):
        used = int((tallies > 0).sum())
        fixed = max(1, used // 4)
        passed = fixed + (places - fixed + offset_by * (used - fixed)) % max(1, number_of - fixed)
        return jnp.zeros((number_of,), jnp.int32).at[sequence[jnp.where(places < fixed, places, passed)]].set(jnp.asarray(tallies, jnp.int32))

    tallies = jnp.where(number % 4 == 0, named(heavy_load, number // 4), named(common, number - number // 4 - 1))
    mixed = jax.random.permutation(jax.random.fold_in(own, 3), number_of)
    giver, sink = mixed[0:number_of // 2 * 2:2], mixed[1:number_of // 2 * 2:2]
    slack = jnp.minimum(tallies[giver] - 1, bound - tallies[sink]) // 2
    slack = jnp.where((giver == sequence[0]) | (sink == sequence[0]) | (tallies[sink] == 0), 0, jnp.maximum(slack, 0))
    passed = jax.random.randint(jax.random.fold_in(own, 4), (number_of // 2,), 0, 1 << 20) % (slack + 1)
    tallies = tallies.at[giver].add(-passed).at[sink].add(passed)
    labels = jnp.searchsorted(jnp.cumsum(tallies), jnp.arange(rows * top), side="right").astype(jnp.int32)
    listing = labels.reshape(top, rows).T
    listing = listing[jax.random.permutation(jax.random.fold_in(own, 1), rows)]
    offset_by = jax.random.randint(jax.random.fold_in(own, 2), (rows, 1), 0, top)
    return jnp.take_along_axis(listing, (jnp.arange(top)[None, :] + offset_by) % top, axis=1)


def load_shares(amount, total, most, skew, full):
    portions = [(1 << 20) // math.isqrt(grade ** skew) + 1 for grade in range(1, amount + 1)]
    largest = most if full else min(most, max(-(-total // amount), total * portions[0] // sum(portions)))
    least = 1 if total - largest >= amount - 1 else 0
    counts, spare = [largest] + [least] * (amount - 1), total - largest - least * (amount - 1)
    while spare > 0:
        movable = [i for i in range(1, amount) if counts[i] < largest] or [i for i in range(1, amount) if counts[i] < most]
        whole, left = sum([portions[i] for i in movable]), spare
        for i in movable:
            more = min(most - counts[i], max(1, left * portions[i] // whole), spare)
            counts[i] = counts[i] + more
            spare = spare - more
    return np.array(counts)


def centred(own_key, extent, deviation, bound, cuts=(), kind=jnp.bfloat16):
    factor_of = levels(own_key, extent, cuts, -0.22, 0.18) if cuts else 1.0
    entries = jax.random.normal(own_key, extent, jnp.float32) * deviation * factor_of
    return jnp.minimum(jnp.maximum(entries, -bound), bound).astype(kind)


def gaussian_with(key, dims, width, bound, shards, heavy, kind=jnp.bfloat16):
    entries = width * jax.random.normal(key, dims, jnp.float32)
    if shards:
        entries = entries * levels(key, dims, shards, -0.22, 0.18)
    return jnp.clip(spiked(entries, jax.random.fold_in(key, 3), *heavy), -bound, bound).astype(kind)


def setup_inputs(seed: int = 0) -> dict:
    key_list = jax.random.split(jax.random.key(seed), 16)
    queries = draw_queries(jax.random.fold_in(key_list[15], 71), 0)
    keys = draw_keys(jax.random.fold_in(key_list[15], 71), 0)
    values = centred(key_list[2], (SEQ, QW), 1.0, 6.0, ((0, 32), (1, 16)))
    cum_gate = draw_cum_gate(jax.random.fold_in(key_list[15], 71), 0)
    head_gain = jnp.clip(1.0 + 0.18 * jax.random.normal(key_list[4], (QW,), jnp.float32), 0.1, 1.9)
    moe_in = centred(key_list[5], (MTOK, D), 1.0, 6.0, ((0, 32),))
    ffn_gain = jnp.clip(1.0 + 0.18 * jax.random.normal(key_list[6], (D,), jnp.float32), 0.1, 1.9)
    routes_keys = jax.random.split(jax.random.fold_in(key_list[7], 1), MTOK // MROWS)
    routes_turns = jax.random.permutation(jax.random.fold_in(key_list[7], 3), MTOK // MROWS)
    routes = jax.vmap(lambda own, number: assign_block(jax.random.fold_in(key_list[7], 2), own, number, MROWS, EXPERTS, TOP, CAP, 2))(routes_keys, routes_turns).reshape((MTOK, TOP))
    route_weight = jnp.clip(0.2 + 1 * jax.random.uniform(key_list[8], (MTOK, TOP), jnp.float32) ** levels(key_list[8], (MTOK, TOP), ((0, 32),), -0.2, 0.2), 0.2, 1.2)
    expert_gate = centred(key_list[9], (EXPERTS, FF_E, D), D ** -0.5, 0.125, ((0, 32), (1, 16)))
    expert_up = centred(key_list[10], (EXPERTS, FF_E, D), D ** -0.5, 0.125, ((0, 32), (1, 16)))
    expert_down = gaussian_with(key_list[11], (EXPERTS, FF_E, D), FF_E ** -0.5, 0.25, ((0, 32), (1, 16)), (1, 2, 16, 2.0))
    shared_gate = centred(key_list[12], (SHARED, D), D ** -0.5, 0.125, ((0, 16),))
    shared_up = centred(key_list[13], (SHARED, D), D ** -0.5, 0.125, ((0, 16),))
    shared_down = gaussian_with(key_list[14], (SHARED, D), SHARED ** -0.5, 0.375, ((0, 16),), (0, 1, 16, 2.0))
    return {"queries": queries, "keys": keys, "values": values, "cum_gate": cum_gate, "head_gain": head_gain, "moe_in": moe_in, "ffn_gain": ffn_gain, "routes": routes, "route_weight": route_weight, "expert_gate": expert_gate, "expert_up": expert_up, "expert_down": expert_down, "shared_gate": shared_gate, "shared_up": shared_up, "shared_down": shared_down}


NORM_EPSILON = 1e-06

def attend_head(head_inputs):
    query_head, key_head, value_head, gate_head = head_inputs
    block_len = math.gcd(SEQ, 512)
    positions = jnp.arange(SEQ, dtype=jnp.int32)
    score_scale = HEAD ** (-0.5)

    def one_block(block_num):
        first_row = block_num * block_len
        query_block = lax.dynamic_slice_in_dim(query_head, first_row, block_len, 0)
        gate_block = lax.dynamic_slice_in_dim(gate_head, first_row, block_len, 0)
        scores = jnp.dot(query_block, key_head.T, preferred_element_type=jnp.float32) * score_scale
        scores = scores + gate_block[:, None] - gate_head[None, :]
        query_pos = first_row + jnp.arange(block_len, dtype=jnp.int32)
        scores = jnp.where(positions[None, :] <= query_pos[:, None], scores, -jnp.inf)
        top_score = lax.optimization_barrier(jnp.max(scores, axis=1, keepdims=True))
        weights = jnp.exp(scores - top_score).astype(jnp.bfloat16)
        return jnp.dot(weights, value_head, preferred_element_type=jnp.float32)
    blocks = lax.map(one_block, jnp.arange(SEQ // block_len, dtype=jnp.int32))
    return blocks.reshape(SEQ, HEAD)

def blocked_down(hidden, weight):
    block_width = hidden.shape[1] // N_TP

    def add_block(running, block_num):
        start_col = block_num * block_width
        product = jnp.dot(lax.dynamic_slice_in_dim(hidden, start_col, block_width, 1), lax.dynamic_slice_in_dim(weight, start_col, block_width, 0), preferred_element_type=jnp.float32)
        rounded = lax.optimization_barrier(product.astype(jnp.bfloat16))
        return (running + rounded.astype(jnp.float32), None)
    start_sum = jnp.zeros((hidden.shape[0], weight.shape[1]), jnp.float32)
    result, _ = lax.scan(add_block, start_sum, jnp.arange(N_TP, dtype=jnp.int32))
    return result

def slot_index(route_rows):
    flat_routes = route_rows.reshape(-1)
    agreement_tally = (flat_routes[:, None] == jnp.arange(EXPERTS, dtype=jnp.int32)[None, :]).astype(jnp.int32)
    earlier = lax.optimization_barrier(jnp.sum((jnp.cumsum(agreement_tally, axis=0) - 1) * agreement_tally, axis=1))
    return (flat_routes * CAP + earlier).astype(jnp.int32)

def fill_slots(token_rows, slot_ids):
    owner_row = jnp.full((EXPERTS * CAP,), MROWS, jnp.int32).at[slot_ids].set(jnp.arange(MROWS * TOP, dtype=jnp.int32) // TOP)
    padded = jnp.concatenate([token_rows, jnp.zeros((1, D), token_rows.dtype)], axis=0)
    return padded[owner_row]

def run_expert(expert_inputs):
    rows_in, gate_weight, up_weight, down_weight = expert_inputs
    hidden = (jax.nn.silu(jnp.dot(rows_in, gate_weight.T, preferred_element_type=jnp.float32)) * jnp.dot(rows_in, up_weight.T, preferred_element_type=jnp.float32)).astype(jnp.bfloat16)
    return blocked_down(hidden, down_weight).astype(jnp.bfloat16)

def reference(queries, keys, values, cum_gate, head_gain, moe_in, ffn_gain, routes, route_weight, expert_gate, expert_up, expert_down, shared_gate, shared_up, shared_down):
    query_heads = queries.reshape(SEQ, HEADS, HEAD).transpose(1, 0, 2)
    key_heads = keys.reshape(SEQ, HEADS, HEAD).transpose(1, 0, 2)
    value_heads = values.reshape(SEQ, HEADS, HEAD).transpose(1, 0, 2)
    summed = lax.map(attend_head, (query_heads, key_heads, value_heads, cum_gate.T))
    mean_square = lax.optimization_barrier(jnp.mean(summed * summed, axis=2, keepdims=True))
    normed_heads = summed * lax.rsqrt(mean_square + NORM_EPSILON) * head_gain.reshape(HEADS, 1, HEAD)
    mixed = normed_heads.transpose(1, 0, 2).reshape(SEQ, QW).astype(jnp.bfloat16)
    source = moe_in.astype(jnp.float32)
    normed = (source * lax.rsqrt(lax.optimization_barrier(jnp.mean(source * source, axis=1, keepdims=True)) + NORM_EPSILON) * ffn_gain).astype(jnp.bfloat16)
    shared_hidden = (jax.nn.silu(jnp.dot(normed, shared_gate.T, preferred_element_type=jnp.float32)) * jnp.dot(normed, shared_up.T, preferred_element_type=jnp.float32)).astype(jnp.bfloat16)
    shared_sum = blocked_down(shared_hidden, shared_down)
    token_blocks = normed.reshape(N_EP, MROWS, D)
    route_blocks = routes.reshape(N_EP, MROWS, TOP)
    slot_ids = jax.vmap(slot_index)(route_blocks)
    buffers = jax.vmap(fill_slots)(token_blocks, slot_ids)
    by_expert = buffers.reshape(N_EP, EXPERTS, CAP, D).transpose(1, 0, 2, 3).reshape(EXPERTS, N_EP * CAP, D)
    results = lax.map(run_expert, (by_expert, expert_gate, expert_up, expert_down))
    returned = results.reshape(EXPERTS, N_EP, CAP, D).transpose(1, 0, 2, 3).reshape(N_EP, EXPERTS * CAP, D)
    picked = returned[jnp.arange(N_EP, dtype=jnp.int32)[:, None], slot_ids]
    picked = picked.reshape(MTOK, TOP, D).astype(jnp.float32)
    routed = lax.optimization_barrier(jnp.sum(picked * route_weight[:, :, None], axis=1))
    expert_out = (shared_sum + routed).astype(jnp.bfloat16)
    return (mixed, expert_out)
```

```python
import functools

import jax
import jax.numpy as jnp
import numpy as np
from jax import lax
from jax.experimental import pallas as pl
from jax.experimental.pallas import tpu as pltpu
from jax.sharding import Mesh
from jax.sharding import PartitionSpec as P


NORM_EPSILON = 1e-06
LOG2E = 1.4426950408889634
NEG = -1e30
NZ, NX, NY, NC = 8, 4, 8, 2
N_EP = NZ * NX
ROWS = 768
HEAD = 64
D = 2048
TOK = 128
CAP = 6
LOCAL = 2
SLOTS = N_EP * LOCAL * CAP
KG = HEAD + 16
KVG = KG + HEAD
F32 = jnp.float32
BF16 = jnp.bfloat16


def wide_slots():
    s = np.arange(2 * SLOTS)
    e, h, j = s // 24, (s % 24) // 12, s % 12
    return e, h, j // CAP, j % CAP


def slot_table():
    e, h, l, p = wide_slots()
    table = np.zeros((2 * SLOTS, 8), np.int32)
    table[:, 0] = 4 * e + l
    table[:, 1] = p
    table[:, 2] = h
    table[:, 3] = l * (SLOTS // 2) + e * CAP + p
    return table


def source_table():
    r = np.arange(SLOTS)
    l, e, p = r // (SLOTS // 2), (r % (SLOTS // 2)) // CAP, r % CAP
    table = np.zeros((SLOTS, 8), np.int32)
    table[:, 0] = e * 24 + l * CAP + p
    table[:, 1] = table[:, 0] + 12
    return table


def dot(a, b):
    return jnp.dot(a, b, preferred_element_type=F32)


def dot_t(a, b):
    return lax.dot_general(a, b, (((1,), (1,)), ((), ())), preferred_element_type=F32)


def three_pieces(v):
    hi = v.astype(BF16)
    rest = v - hi.astype(F32)
    mid = rest.astype(BF16)
    lo = (rest - mid.astype(F32)).astype(BF16)
    return hi, mid, lo


def call(body, out_shape, scalars, grid, in_specs, out_specs, args, scratch=(), flops=0, aliases=None):
    return pl.pallas_call(
        body,
        out_shape=out_shape,
        grid_spec=pltpu.PrefetchScalarGridSpec(
            num_scalar_prefetch=1,
            grid=grid,
            in_specs=in_specs,
            out_specs=out_specs,
            scratch_shapes=list(scratch),
        ),
        compiler_params=pltpu.CompilerParams(
            dimension_semantics=("arbitrary",) * len(grid), vmem_limit_bytes=56 * 2**20
        ),
        input_output_aliases=aliases or {},
        cost_estimate=pl.CostEstimate(flops=flops, bytes_accessed=4 << 20, transcendentals=0),
    )(scalars, *args)


def whole(shape):
    return pl.BlockSpec(shape, lambda i, s: (0,) * len(shape))


UNREAD = pl.BlockSpec(memory_space=pl.ANY)


def pack_body(ids, k_ref, v_ref, g_ref, out_ref):
    out_ref[0:HEAD, :] = k_ref[...]
    out_ref[KG:KVG, :] = v_ref[...]
    hi, mid, lo = three_pieces(g_ref[...] * (-LOG2E))
    row = lax.broadcasted_iota(jnp.int32, (16, ROWS), 0)
    zero = jnp.zeros((16, ROWS), F32)
    pieces = jnp.where(
        row == 0,
        hi.astype(F32),
        jnp.where(row == 1, mid.astype(F32), jnp.where(row == 2, lo.astype(F32), zero)),
    )
    out_ref[HEAD:KG, :] = pieces.astype(BF16)


def trade_body(ids, gate_ref, up_ref, down_ref, sgate_ref, sup_ref, sdown_ref, after_ref, out_ref):
    for i, ref in enumerate((gate_ref, up_ref, down_ref)):
        for l in range(LOCAL):
            out_ref[i * 128 + l * 64 : i * 128 + l * 64 + 64, :] = ref[l]
    for i, ref in enumerate((sgate_ref, sup_ref, sdown_ref)):
        out_ref[384 + i * 32 : 416 + i * 32, :] = ref[...]


QT = 384
DEPTH = 2 * HEAD + 16


def attend_body(turns, ids, q0_ref, q1_ref, kvg_ref, out0_ref, out1_ref, ka_ref):
    z, x = ids[0], ids[1]
    step = pl.program_id(0)
    per = ROWS // QT
    early = step < per
    sub = lax.rem(step, per)
    xq = lax.rem(x + jnp.where(early, turns[0], turns[1]), NX)

    @pl.when(step == 0)
    def _():
        ka_ref[:, 0:HEAD, :] = kvg_ref[:, 0:HEAD, :]
        ka_ref[:, HEAD:DEPTH, :] = kvg_ref[:, 0:KG, :]

    q0, q1 = q0_ref[...].astype(F32), q1_ref[...].astype(F32)
    scaled = jnp.where(early, q0, q1).T * (0.125 * LOG2E)
    hi = scaled.astype(BF16)
    lo = (scaled - hi.astype(F32)).astype(BF16)
    qa = jnp.concatenate([hi, lo, jnp.ones((QT, 16), BF16)], axis=1)

    def update(chunk, carry, masked):
        peak, acc = carry
        s = dot(qa, ka_ref[chunk])
        if masked:
            row = lax.broadcasted_iota(jnp.int32, (QT, ROWS), 0) + sub * QT
            col = lax.broadcasted_iota(jnp.int32, (QT, ROWS), 1)
            s = jnp.where(col <= row, s, NEG)
        new_peak = jnp.maximum(peak, jnp.max(s, axis=1, keepdims=True))
        w = jnp.exp2(s - new_peak).astype(BF16)
        acc = acc * jnp.exp2(peak - new_peak) + dot_t(w, kvg_ref[chunk, KG:KVG, :])
        return new_peak, acc

    start = (jnp.full((QT, 1), NEG, F32), jnp.zeros((QT, HEAD), F32))
    full = jnp.where(xq > x, z + 1, z)
    carry = lax.fori_loop(0, full, lambda i, c: update(i, c, False), start)
    peak, acc = lax.cond(xq == x, lambda c: update(z, c, True), lambda c: c, carry)
    p_hi, p_mid, p_lo = three_pieces(peak)
    lane = lax.broadcasted_iota(jnp.int32, (QT, HEAD), 1)
    tail = jnp.where(
        lane == 0,
        p_hi.astype(F32),
        jnp.where(
            lane == 1, p_mid.astype(F32), jnp.where(lane == 2, p_lo.astype(F32), jnp.zeros((), F32))
        ),
    )
    out = jnp.concatenate([acc, tail], axis=1).astype(BF16)
    at = pl.ds(pl.multiple_of(sub * QT, QT), QT)

    @pl.when(early)
    def _():
        out0_ref[at, :] = out

    @pl.when(jnp.logical_not(early))
    def _():
        out1_ref[at, :] = out


def combine_body(ids, gain_ref, *refs):
    out_ref, parts = refs[-1], refs[:-1]
    peaks = []
    for ref in parts:
        tail = ref[:, HEAD : HEAD + 3].astype(F32)
        peaks.append(tail[:, 0:1] + tail[:, 1:2] + tail[:, 2:3])
    top = jnp.maximum(jnp.maximum(peaks[0], peaks[1]), jnp.maximum(peaks[2], peaks[3]))
    total = jnp.zeros((ROWS, HEAD), F32)
    for ref, peak in zip(parts, peaks):
        total = total + ref[:, 0:HEAD].astype(F32) * jnp.exp2(peak - top)
    mean_square = jnp.mean(total * total, axis=1, keepdims=True)
    out = total * lax.rsqrt(mean_square + NORM_EPSILON) * gain_ref[...]
    out_ref[...] = out.T.astype(BF16)


def dispatch_body(ids, x_ref, gain_ref, routes_ref, table_ref, after_ref, normed_ref, send_ref):
    c = ids[2]
    x = x_ref[...].astype(F32)
    mean_square = jnp.mean(x * x, axis=1, keepdims=True)
    normed = (x * lax.rsqrt(mean_square + NORM_EPSILON) * gain_ref[...]).astype(BF16)
    normed_ref[...] = normed
    expert = table_ref[:, 0:1] + 2 * c
    member = jnp.zeros((2 * SLOTS, TOK), F32)
    for k in range(4):
        member = jnp.where(routes_ref[k : k + 1, :] == expert, 1.0, member)
    before = lax.broadcasted_iota(jnp.int32, (TOK, TOK), 0)
    after = lax.broadcasted_iota(jnp.int32, (TOK, TOK), 1)
    earlier = jnp.where(before < after, 1.0, 0.0).astype(BF16)
    rank = dot(member.astype(BF16), earlier)
    pick = jnp.where(rank == table_ref[:, 1:2].astype(F32), member, 0.0)
    half = table_ref[:, 2:3]
    first = jnp.where(half == 0, pick, 0.0).astype(BF16)
    second = jnp.where(half == 1, pick, 0.0).astype(BF16)
    send_ref[...] = (dot(first, normed[:, : D // 2]) + dot(second, normed[:, D // 2 :])).astype(
        BF16
    )


def split_down_body(ids, own_ref, got_ref, shared_ref, *outs):
    for turn, out_ref in enumerate(outs):
        to = lax.rem(ids[3] + turn, NY)
        cols = pl.ds(pl.multiple_of(to * 256, 256), 256)
        for l in range(LOCAL):
            out_ref[l * 128 : l * 128 + 64, :] = own_ref[l, :, cols]
            out_ref[l * 128 + 64 : l * 128 + 128, :] = got_ref[256 + l * 64 : 320 + l * 64, cols]
        out_ref[256:288, :] = shared_ref[:, cols]
        out_ref[288:320, :] = got_ref[448:480, cols]


def gated(g, u):
    return g / (1.0 + jnp.exp(-g)) * u


def hidden_body(
    ids, x_ref, gate_ref, up_ref, got_ref, normed_ref, sgate_ref, sup_ref, source_ref, out_ref
):
    c = ids[2]
    x = x_ref[...]
    lane = lax.broadcasted_iota(jnp.int32, (SLOTS, 2 * SLOTS), 1)
    x0 = dot(jnp.where(lane == source_ref[:, 0:1], 1.0, 0.0).astype(BF16), x).astype(BF16)
    x1 = dot(jnp.where(lane == source_ref[:, 1:2], 1.0, 0.0).astype(BF16), x).astype(BF16)
    n = SLOTS // 2
    for l in range(LOCAL):
        rows0, rows1 = x0[l * n : (l + 1) * n], x1[l * n : (l + 1) * n]
        wg = jnp.concatenate([gate_ref[l], got_ref[l * 64 : l * 64 + 64, :]], axis=0)
        wu = jnp.concatenate([up_ref[l], got_ref[128 + l * 64 : 128 + l * 64 + 64, :]], axis=0)
        g = dot_t(rows0, wg[:, : D // 2]) + dot_t(rows1, wg[:, D // 2 :])
        u = dot_t(rows0, wu[:, : D // 2]) + dot_t(rows1, wu[:, D // 2 :])
        h = gated(g, u).astype(BF16)
        for y in range(NY):
            out_ref[y, l * n : (l + 1) * n, :] = h
    tokens = normed_ref[pl.ds(pl.multiple_of(c * 64, 64), 64), :]
    wg = jnp.concatenate([sgate_ref[...], got_ref[384:416, :]], axis=0)
    wu = jnp.concatenate([sup_ref[...], got_ref[416:448, :]], axis=0)
    h = gated(dot_t(tokens, wg), dot_t(tokens, wu))
    h = jnp.concatenate([h, jnp.zeros((64, 64), F32)], axis=1).astype(BF16)
    for y in range(NY):
        out_ref[y, SLOTS : SLOTS + 64, :] = h


def down_body(ids, h_ref, table_ref, *rest):
    weights, (out_ref, shared_ref) = rest[:NY], rest[NY:]
    n = SLOTS // 2
    rows = [jnp.zeros((n, 256), F32) for _ in range(LOCAL)]
    shared = jnp.zeros((64, 256), F32)
    for turn, w_ref in enumerate(weights):
        y = lax.rem(ids[3] + NY - turn, NY)
        h = h_ref[y]
        for l in range(LOCAL):
            rows[l] = rows[l] + dot(h[l * n : (l + 1) * n], w_ref[l * 128 : l * 128 + 128, :])
        shared = shared + dot(h[SLOTS : SLOTS + 64, 0:64], w_ref[256:320, :])
    rows = [r.astype(BF16) for r in rows]
    shared_ref[...] = shared
    rows = jnp.concatenate(rows, axis=0)
    lane = lax.broadcasted_iota(jnp.int32, (2 * SLOTS, SLOTS), 1)
    place = jnp.where(lane == table_ref[:, 3:4], 1.0, 0.0)
    half = table_ref[:, 2:3]
    first = jnp.where(half == 0, place, 0.0).astype(BF16)
    second = jnp.where(half == 1, place, 0.0).astype(BF16)
    out_ref[...] = (dot(first, rows[:, :128]) + dot(second, rows[:, 128:])).astype(BF16)


def weigh_body(ids, y_ref, routes_ref, weight_ref, table_ref, shared_ref, own_ref, send_ref):
    c = ids[2]
    expert = table_ref[0:1, :] + 2 * c
    member = jnp.zeros((TOK, 2 * SLOTS), F32)
    weight = jnp.zeros((TOK, 2 * SLOTS), F32)
    for k in range(4):
        same = routes_ref[:, k : k + 1] == expert
        member = jnp.where(same, 1.0, member)
        weight = jnp.where(same, weight_ref[:, k : k + 1], weight)
    after = lax.broadcasted_iota(jnp.int32, (TOK, TOK), 0)
    before = lax.broadcasted_iota(jnp.int32, (TOK, TOK), 1)
    earlier = jnp.where(before < after, 1.0, 0.0).astype(BF16)
    rank = dot(earlier, member.astype(BF16))
    weight = jnp.where(rank == table_ref[1:2, :].astype(F32), weight, 0.0)
    half = table_ref[2:3, :]
    y = y_ref[...]
    row = lax.broadcasted_iota(jnp.int32, (TOK, 128), 0)
    mine = (row >= c * 64) & (row < c * 64 + 64)
    shared = shared_ref[...]
    shared = jnp.concatenate([shared, shared], axis=0)
    for which, ref in ((c, own_ref), (1 - c, send_ref)):
        part = jnp.where(half == which, weight, 0.0)
        total = jnp.zeros((TOK, 128), F32)
        for piece in three_pieces(part):
            total = total + dot(piece, y)
        columns = jnp.where(which == 0, shared[:, :128], shared[:, 128:])
        ref[...] = total + jnp.where(mine, columns, 0.0)


def on_device(
    queries,
    keys,
    values,
    cum_gate,
    head_gain,
    moe_in,
    ffn_gain,
    routes,
    route_weight,
    expert_gate,
    expert_up,
    expert_down,
    shared_gate,
    shared_up,
    shared_down,
):
    z, x, y, c = (lax.axis_index(a) for a in ("z", "x", "y", "c"))
    ids = jnp.stack([z, x, c, y]).astype(jnp.int32)
    table = jnp.asarray(slot_table())
    source = jnp.asarray(source_table())
    swap = [(0, 1), (1, 0)]

    packed = call(
        pack_body,
        jax.ShapeDtypeStruct((KVG, ROWS), BF16),
        ids,
        (1,),
        [whole((HEAD, ROWS)), whole((HEAD, ROWS)), whole((1, ROWS))],
        whole((KVG, ROWS)),
        (keys.T, values.T, cum_gate.reshape(1, ROWS)),
    )
    kvg = lax.all_gather(packed, "z", axis=0, tiled=True).reshape(NZ, KVG, ROWS)

    normed, sent = call(
        dispatch_body,
        (
            jax.ShapeDtypeStruct((TOK, D), BF16),
            jax.ShapeDtypeStruct((2 * SLOTS, D // 2), BF16),
        ),
        ids,
        (1,),
        [whole((TOK, D)), whole((1, D)), whole((4, TOK)), whole((2 * SLOTS, 8)), UNREAD],
        (whole((TOK, D)), whole((2 * SLOTS, D // 2))),
        (moe_in, ffn_gain.reshape(1, D), routes.T, table, packed),
        flops=1_000_000_000,
    )
    arrived = lax.all_to_all(sent, ("z", "x"), 0, 0, tiled=True)

    other = pl.BlockSpec((LOCAL, 64, D), lambda i, s: (1 - s[2], 0, 0))
    trade = call(
        trade_body,
        jax.ShapeDtypeStruct((480, D), BF16),
        ids,
        (1,),
        [other, other, other, whole((32, D)), whole((32, D)), whole((32, D)), UNREAD],
        whole((480, D)),
        (expert_gate, expert_up, expert_down, shared_gate, shared_up, shared_down, sent),
        flops=1_000_000_000,
    )
    got = lax.ppermute(trade, "c", swap)

    mine, _ = lax.optimization_barrier((queries.T, trade))
    q_all = [mine] + [
        lax.ppermute(mine, "x", [((i + d) % NX, i) for i in range(NX)]) for d in range(1, NX)
    ]

    down_sent = call(
        split_down_body,
        (jax.ShapeDtypeStruct((320, 256), BF16),) * NY,
        ids,
        (1,),
        [pl.BlockSpec((LOCAL, 64, D), lambda i, s: (s[2], 0, 0)), whole((480, D)), whole((32, D))],
        (whole((320, 256)),) * NY,
        (expert_down, got, shared_down),
        flops=1_000_000_000,
    )
    down = [down_sent[0]] + [
        lax.ppermute(down_sent[r], "y", [(i, (i + r) % NY) for i in range(NY)])
        for r in range(1, NY)
    ]

    hidden_sent = call(
        hidden_body,
        jax.ShapeDtypeStruct((NY, SLOTS + 64, 128), BF16),
        ids,
        (1,),
        [
            whole((2 * SLOTS, D // 2)),
            pl.BlockSpec((LOCAL, 64, D), lambda i, s: (s[2], 0, 0)),
            pl.BlockSpec((LOCAL, 64, D), lambda i, s: (s[2], 0, 0)),
            whole((480, D)),
            whole((TOK, D)),
            whole((32, D)),
            whole((32, D)),
            whole((SLOTS, 8)),
        ],
        whole((NY, SLOTS + 64, 128)),
        (arrived, expert_gate, expert_up, got, normed, shared_gate, shared_up, source),
        flops=1_000_000_000,
    )
    hidden = lax.all_to_all(hidden_sent, "y", 0, 0, tiled=True)

    def attend(turns):
        return call(
            functools.partial(attend_body, turns),
            (jax.ShapeDtypeStruct((ROWS, 128), BF16),) * 2,
            ids,
            (2 * (ROWS // QT),),
            [pl.BlockSpec((HEAD, QT), lambda i, s: (0, lax.rem(i, ROWS // QT)))] * 2
            + [whole((NZ, KVG, ROWS))],
            (whole((ROWS, 128)),) * 2,
            (q_all[turns[0]], q_all[turns[1]], kvg),
            scratch=[pltpu.VMEM((NZ, DEPTH, ROWS), BF16)],
            flops=10_000_000_000,
        )

    def send_part(part, d):
        return lax.ppermute(part, "x", [(i, (i + d) % NX) for i in range(NX)])

    part1, part2 = attend((1, 2))
    part1, part2 = send_part(part1, 1), send_part(part2, 2)

    rows, shared = call(
        down_body,
        (
            jax.ShapeDtypeStruct((2 * SLOTS, 128), BF16),
            jax.ShapeDtypeStruct((64, 256), F32),
        ),
        ids,
        (1,),
        [whole((NY, SLOTS + 64, 128)), whole((2 * SLOTS, 8))] + [whole((320, 256))] * NY,
        (whole((2 * SLOTS, 128)), whole((64, 256))),
        (hidden, table, *down),
        flops=1_000_000_000,
    )
    returned = lax.all_to_all(rows, ("z", "x"), 0, 0, tiled=True)

    part3, part0 = attend((3, 0))
    part3 = send_part(part3, 3)

    mixed = call(
        combine_body,
        jax.ShapeDtypeStruct((HEAD, ROWS), BF16),
        ids,
        (1,),
        [whole((1, HEAD))] + [whole((ROWS, 128))] * NX,
        whole((HEAD, ROWS)),
        (head_gain.reshape(1, HEAD), part0, part1, part2, part3),
    ).T

    own, give = call(
        weigh_body,
        (jax.ShapeDtypeStruct((TOK, 128), F32), jax.ShapeDtypeStruct((TOK, 128), F32)),
        ids,
        (1,),
        [
            whole((2 * SLOTS, 128)),
            whole((TOK, 4)),
            whole((TOK, 4)),
            whole((8, 2 * SLOTS)),
            whole((64, 256)),
        ],
        (whole((TOK, 128)), whole((TOK, 128))),
        (returned, routes, route_weight, table.T, shared),
        flops=1_000_000_000,
    )
    taken = lax.ppermute(give, "c", swap)
    expert_out = (own + taken).astype(BF16)
    return (mixed, expert_out)


def solution(mesh):
    fine = Mesh(mesh.devices.reshape(NZ, NX, NY, NC), ("z", "x", "y", "c"))
    ep, tp = ("z", "x"), ("y", "c")
    in_specs = (
        P(ep, tp),
        P(ep, tp),
        P(ep, tp),
        P(ep, tp),
        P(tp),
        P(ep, None),
        P(),
        P(ep, None),
        P(ep, None),
        P(ep, tp, None),
        P(ep, tp, None),
        P(ep, tp, None),
        P(tp, None),
        P(tp, None),
        P(tp, None),
    )
    out_specs = (P(ep, tp), P(ep, tp))

    return jax.shard_map(
        on_device, mesh=fine, in_specs=in_specs, out_specs=out_specs, check_vma=False
    )
```

```python
import functools

import jax
import jax.numpy as jnp
import numpy as np
from jax import lax
from jax.experimental import pallas as pl
from jax.experimental.pallas import tpu as pltpu
from jax.sharding import Mesh
from jax.sharding import PartitionSpec as P


NORM_EPSILON = 1e-06
LOG2E = 1.4426950408889634
NEG = -1e30
NZ, NX, NY, NC = 8, 4, 8, 2
N_EP = NZ * NX
ROWS = 768
HEAD = 64
D = 2048
TOK = 128
CAP = 6
LOCAL = 2
SLOTS = N_EP * LOCAL * CAP
KG = HEAD + 16
KVG = KG + HEAD
F32 = jnp.float32
BF16 = jnp.bfloat16


def wide_slots():
    s = np.arange(2 * SLOTS)
    e, h, j = s // 24, (s % 24) // 12, s % 12
    return e, h, j // CAP, j % CAP


def slot_table():
    e, h, l, p = wide_slots()
    table = np.zeros((2 * SLOTS, 8), np.int32)
    table[:, 0] = 4 * e + l
    table[:, 1] = p
    table[:, 2] = h
    table[:, 3] = l * (SLOTS // 2) + e * CAP + p
    return table


def source_table():
    r = np.arange(SLOTS)
    l, e, p = r // (SLOTS // 2), (r % (SLOTS // 2)) // CAP, r % CAP
    table = np.zeros((SLOTS, 8), np.int32)
    table[:, 0] = e * 24 + l * CAP + p
    table[:, 1] = table[:, 0] + 12
    return table


def dot(a, b):
    return jnp.dot(a, b, preferred_element_type=F32)


def dot_t(a, b):
    return lax.dot_general(a, b, (((1,), (1,)), ((), ())), preferred_element_type=F32)


def three_pieces(v):
    hi = v.astype(BF16)
    rest = v - hi.astype(F32)
    mid = rest.astype(BF16)
    lo = (rest - mid.astype(F32)).astype(BF16)
    return hi, mid, lo


def call(body, out_shape, scalars, grid, in_specs, out_specs, args, scratch=(), flops=0, aliases=None):
    return pl.pallas_call(
        body,
        out_shape=out_shape,
        grid_spec=pltpu.PrefetchScalarGridSpec(
            num_scalar_prefetch=1,
            grid=grid,
            in_specs=in_specs,
            out_specs=out_specs,
            scratch_shapes=list(scratch),
        ),
        compiler_params=pltpu.CompilerParams(
            dimension_semantics=("arbitrary",) * len(grid), vmem_limit_bytes=56 * 2**20
        ),
        input_output_aliases=aliases or {},
        cost_estimate=pl.CostEstimate(flops=flops, bytes_accessed=4 << 20, transcendentals=0),
    )(scalars, *args)


def whole(shape):
    return pl.BlockSpec(shape, lambda i, s: (0,) * len(shape))


UNREAD = pl.BlockSpec(memory_space=pl.ANY)


def pack_body(ids, k_ref, v_ref, g_ref, out_ref):
    out_ref[0:HEAD, :] = k_ref[...]
    out_ref[KG:KVG, :] = v_ref[...]
    hi, mid, lo = three_pieces(g_ref[...] * (-LOG2E))
    row = lax.broadcasted_iota(jnp.int32, (16, ROWS), 0)
    zero = jnp.zeros((16, ROWS), F32)
    pieces = jnp.where(
        row == 0,
        hi.astype(F32),
        jnp.where(row == 1, mid.astype(F32), jnp.where(row == 2, lo.astype(F32), zero)),
    )
    out_ref[HEAD:KG, :] = pieces.astype(BF16)


def trade_body(ids, gate_ref, up_ref, down_ref, sgate_ref, sup_ref, sdown_ref, after_ref, out_ref):
    for i, ref in enumerate((gate_ref, up_ref, down_ref)):
        for l in range(LOCAL):
            out_ref[i * 128 + l * 64 : i * 128 + l * 64 + 64, :] = ref[l]
    for i, ref in enumerate((sgate_ref, sup_ref, sdown_ref)):
        out_ref[384 + i * 32 : 416 + i * 32, :] = ref[...]


TILE = 384
TILES = ROWS // TILE
DEPTH = 2 * HEAD + 16


def attend_body(turns, ids, q0_ref, q1_ref, kvg_ref, out0_ref, out1_ref, ka_ref):
    z, x = ids[0], ids[1]
    ka_ref[:, 0:HEAD, :] = kvg_ref[:, 0:HEAD, :]
    ka_ref[:, HEAD:DEPTH, :] = kvg_ref[:, 0:KG, :]
    tiles = []
    for ref in (q0_ref, q1_ref):
        scaled = ref[...].astype(F32).T * (0.125 * LOG2E)
        hi = scaled.astype(BF16)
        lo = (scaled - hi.astype(F32)).astype(BF16)
        rows = jnp.concatenate([hi, lo, jnp.ones((ROWS, 16), BF16)], axis=1)
        tiles += [rows[i * TILE : (i + 1) * TILE] for i in range(TILES)]

    def weigh(s, values, peak, acc):
        new_peak = jnp.maximum(peak, jnp.max(s, axis=1, keepdims=True))
        w = jnp.exp2(s - new_peak).astype(BF16)
        return new_peak, acc * jnp.exp2(peak - new_peak) + dot_t(w, values)

    def update(chunk, carry, some, masked):
        k, values = ka_ref[chunk], kvg_ref[chunk, KG:KVG, :]
        scores = [dot(tile, k) for tile in some]
        if masked:
            for i in range(TILES):
                row = lax.broadcasted_iota(jnp.int32, (TILE, ROWS), 0) + i * TILE
                col = lax.broadcasted_iota(jnp.int32, (TILE, ROWS), 1)
                scores[i] = jnp.where(col <= row, scores[i], NEG)
        return tuple(weigh(s, values, *c) for s, c in zip(scores, carry))

    start = ((jnp.full((TILE, 1), NEG, F32), jnp.zeros((TILE, HEAD), F32)),) * (2 * TILES)
    carry = lax.fori_loop(0, z, lambda i, c: update(i, c, tiles, False), start)
    lane = lax.broadcasted_iota(jnp.int32, (ROWS, HEAD), 1)
    for n, (turn, ref) in enumerate(zip(turns, (out0_ref, out1_ref))):
        mine = slice(n * TILES, (n + 1) * TILES)
        if turn == 0:
            last = update(z, carry[mine], tiles[mine], True)
        else:
            last = lax.cond(
                lax.rem(x + turn, NX) > x,
                lambda c, some=tiles[mine]: update(z, c, some, False),
                lambda c: c,
                carry[mine],
            )
        acc = jnp.concatenate([c[1] for c in last], axis=0)
        p_hi, p_mid, p_lo = three_pieces(jnp.concatenate([c[0] for c in last], axis=0))
        tail = jnp.where(
            lane == 0,
            p_hi.astype(F32),
            jnp.where(
                lane == 1,
                p_mid.astype(F32),
                jnp.where(lane == 2, p_lo.astype(F32), jnp.zeros((), F32)),
            ),
        )
        ref[...] = jnp.concatenate([acc, tail], axis=1).astype(BF16)


def combine_body(ids, gain_ref, *refs):
    out_ref, parts = refs[-1], refs[:-1]
    peaks = []
    for ref in parts:
        tail = ref[:, HEAD : HEAD + 3].astype(F32)
        peaks.append(tail[:, 0:1] + tail[:, 1:2] + tail[:, 2:3])
    top = jnp.maximum(jnp.maximum(peaks[0], peaks[1]), jnp.maximum(peaks[2], peaks[3]))
    total = jnp.zeros((ROWS, HEAD), F32)
    for ref, peak in zip(parts, peaks):
        total = total + ref[:, 0:HEAD].astype(F32) * jnp.exp2(peak - top)
    mean_square = jnp.mean(total * total, axis=1, keepdims=True)
    out = total * lax.rsqrt(mean_square + NORM_EPSILON) * gain_ref[...]
    out_ref[...] = out.T.astype(BF16)


def dispatch_body(ids, x_ref, gain_ref, routes_ref, table_ref, after_ref, normed_ref, send_ref):
    c = ids[2]
    x = x_ref[...].astype(F32)
    mean_square = jnp.mean(x * x, axis=1, keepdims=True)
    normed = (x * lax.rsqrt(mean_square + NORM_EPSILON) * gain_ref[...]).astype(BF16)
    normed_ref[...] = normed
    expert = table_ref[:, 0:1] + 2 * c
    member = jnp.zeros((2 * SLOTS, TOK), F32)
    for k in range(4):
        member = jnp.where(routes_ref[k : k + 1, :] == expert, 1.0, member)
    before = lax.broadcasted_iota(jnp.int32, (TOK, TOK), 0)
    after = lax.broadcasted_iota(jnp.int32, (TOK, TOK), 1)
    earlier = jnp.where(before < after, 1.0, 0.0).astype(BF16)
    rank = dot(member.astype(BF16), earlier)
    pick = jnp.where(rank == table_ref[:, 1:2].astype(F32), member, 0.0)
    half = table_ref[:, 2:3]
    first = jnp.where(half == 0, pick, 0.0).astype(BF16)
    second = jnp.where(half == 1, pick, 0.0).astype(BF16)
    send_ref[...] = (dot(first, normed[:, : D // 2]) + dot(second, normed[:, D // 2 :])).astype(
        BF16
    )


def gated(g, u):
    return g / (1.0 + jnp.exp(-g)) * u


def experts_body(
    ids,
    x_ref,
    gate_ref,
    up_ref,
    down_ref,
    got_ref,
    normed_ref,
    sgate_ref,
    sup_ref,
    sdown_ref,
    source_ref,
    out_ref,
):
    c = ids[2]
    x = x_ref[...]
    lane = lax.broadcasted_iota(jnp.int32, (SLOTS, 2 * SLOTS), 1)
    x0 = dot(jnp.where(lane == source_ref[:, 0:1], 1.0, 0.0).astype(BF16), x).astype(BF16)
    x1 = dot(jnp.where(lane == source_ref[:, 1:2], 1.0, 0.0).astype(BF16), x).astype(BF16)
    n = SLOTS // 2
    for l in range(LOCAL):
        rows0, rows1 = x0[l * n : (l + 1) * n], x1[l * n : (l + 1) * n]
        wg = jnp.concatenate([gate_ref[l], got_ref[l * 64 : l * 64 + 64, :]], axis=0)
        wu = jnp.concatenate([up_ref[l], got_ref[128 + l * 64 : 128 + l * 64 + 64, :]], axis=0)
        g = dot_t(rows0, wg[:, : D // 2]) + dot_t(rows1, wg[:, D // 2 :])
        u = dot_t(rows0, wu[:, : D // 2]) + dot_t(rows1, wu[:, D // 2 :])
        h = gated(g, u).astype(BF16)
        wd = jnp.concatenate([down_ref[l], got_ref[256 + l * 64 : 320 + l * 64, :]], axis=0)
        for y in range(NY):
            out_ref[y, l * n : (l + 1) * n, :] = dot(h, wd[:, y * 256 : y * 256 + 256]).astype(BF16)
    tokens = normed_ref[pl.ds(pl.multiple_of(c * 64, 64), 64), :]
    wg = jnp.concatenate([sgate_ref[...], got_ref[384:416, :]], axis=0)
    wu = jnp.concatenate([sup_ref[...], got_ref[416:448, :]], axis=0)
    h = gated(dot_t(tokens, wg), dot_t(tokens, wu)).astype(BF16)
    wd = jnp.concatenate([sdown_ref[...], got_ref[448:480, :]], axis=0)
    for y in range(NY):
        part = dot(h, wd[:, y * 256 : y * 256 + 256])
        out_ref[y, SLOTS : SLOTS + 64, :] = part.astype(BF16)


def sum_body(ids, part_ref, table_ref, out_ref, shared_ref):
    total = jnp.zeros((SLOTS + 64, 256), F32)
    for y in range(NY):
        total = total + part_ref[y].astype(F32)
    shared_ref[...] = total[SLOTS:]
    rows = total[:SLOTS].astype(BF16)
    lane = lax.broadcasted_iota(jnp.int32, (2 * SLOTS, SLOTS), 1)
    place = jnp.where(lane == table_ref[:, 3:4], 1.0, 0.0)
    half = table_ref[:, 2:3]
    first = jnp.where(half == 0, place, 0.0).astype(BF16)
    second = jnp.where(half == 1, place, 0.0).astype(BF16)
    out_ref[...] = (dot(first, rows[:, :128]) + dot(second, rows[:, 128:])).astype(BF16)


def weigh_body(ids, y_ref, routes_ref, weight_ref, table_ref, shared_ref, own_ref, send_ref):
    c = ids[2]
    expert = table_ref[0:1, :] + 2 * c
    member = jnp.zeros((TOK, 2 * SLOTS), F32)
    weight = jnp.zeros((TOK, 2 * SLOTS), F32)
    for k in range(4):
        same = routes_ref[:, k : k + 1] == expert
        member = jnp.where(same, 1.0, member)
        weight = jnp.where(same, weight_ref[:, k : k + 1], weight)
    after = lax.broadcasted_iota(jnp.int32, (TOK, TOK), 0)
    before = lax.broadcasted_iota(jnp.int32, (TOK, TOK), 1)
    earlier = jnp.where(before < after, 1.0, 0.0).astype(BF16)
    rank = dot(earlier, member.astype(BF16))
    weight = jnp.where(rank == table_ref[1:2, :].astype(F32), weight, 0.0)
    half = table_ref[2:3, :]
    y = y_ref[...]
    row = lax.broadcasted_iota(jnp.int32, (TOK, 128), 0)
    mine = (row >= c * 64) & (row < c * 64 + 64)
    shared = shared_ref[...]
    shared = jnp.concatenate([shared, shared], axis=0)
    for which, ref in ((c, own_ref), (1 - c, send_ref)):
        part = jnp.where(half == which, weight, 0.0)
        total = jnp.zeros((TOK, 128), F32)
        for piece in three_pieces(part):
            total = total + dot(piece, y)
        columns = jnp.where(which == 0, shared[:, :128], shared[:, 128:])
        ref[...] = total + jnp.where(mine, columns, 0.0)


def on_device(
    queries,
    keys,
    values,
    cum_gate,
    head_gain,
    moe_in,
    ffn_gain,
    routes,
    route_weight,
    expert_gate,
    expert_up,
    expert_down,
    shared_gate,
    shared_up,
    shared_down,
):
    z, x, y, c = (lax.axis_index(a) for a in ("z", "x", "y", "c"))
    ids = jnp.stack([z, x, c, y]).astype(jnp.int32)
    table = jnp.asarray(slot_table())
    source = jnp.asarray(source_table())
    swap = [(0, 1), (1, 0)]

    packed = call(
        pack_body,
        jax.ShapeDtypeStruct((KVG, ROWS), BF16),
        ids,
        (1,),
        [whole((HEAD, ROWS)), whole((HEAD, ROWS)), whole((1, ROWS))],
        whole((KVG, ROWS)),
        (keys.T, values.T, cum_gate.reshape(1, ROWS)),
    )
    kvg = lax.all_gather(packed, "z", axis=0, tiled=True).reshape(NZ, KVG, ROWS)

    normed, sent = call(
        dispatch_body,
        (
            jax.ShapeDtypeStruct((TOK, D), BF16),
            jax.ShapeDtypeStruct((2 * SLOTS, D // 2), BF16),
        ),
        ids,
        (1,),
        [whole((TOK, D)), whole((1, D)), whole((4, TOK)), whole((2 * SLOTS, 8)), UNREAD],
        (whole((TOK, D)), whole((2 * SLOTS, D // 2))),
        (moe_in, ffn_gain.reshape(1, D), routes.T, table, packed),
        flops=1_000_000_000,
    )
    arrived = lax.all_to_all(sent, ("z", "x"), 0, 0, tiled=True)

    other = pl.BlockSpec((LOCAL, 64, D), lambda i, s: (1 - s[2], 0, 0))
    trade = call(
        trade_body,
        jax.ShapeDtypeStruct((480, D), BF16),
        ids,
        (1,),
        [other, other, other, whole((32, D)), whole((32, D)), whole((32, D)), UNREAD],
        whole((480, D)),
        (expert_gate, expert_up, expert_down, shared_gate, shared_up, shared_down, sent),
        flops=1_000_000_000,
    )
    got = lax.ppermute(trade, "c", swap)

    mine, _ = lax.optimization_barrier((queries.T, trade))
    q_all = [mine] + [
        lax.ppermute(mine, "x", [((i + d) % NX, i) for i in range(NX)]) for d in range(1, NX)
    ]

    mine = pl.BlockSpec((LOCAL, 64, D), lambda i, s: (s[2], 0, 0))
    products = call(
        experts_body,
        jax.ShapeDtypeStruct((NY, SLOTS + 64, 256), BF16),
        ids,
        (1,),
        [
            whole((2 * SLOTS, D // 2)),
            mine,
            mine,
            mine,
            whole((480, D)),
            whole((TOK, D)),
            whole((32, D)),
            whole((32, D)),
            whole((32, D)),
            whole((SLOTS, 8)),
        ],
        whole((NY, SLOTS + 64, 256)),
        (
            arrived,
            expert_gate,
            expert_up,
            expert_down,
            got,
            normed,
            shared_gate,
            shared_up,
            shared_down,
            source,
        ),
        flops=1_000_000_000,
    )
    products = lax.all_to_all(products, "y", 0, 0, tiled=True)

    def attend(turns):
        return call(
            functools.partial(attend_body, turns),
            (jax.ShapeDtypeStruct((ROWS, 128), BF16),) * 2,
            ids,
            (1,),
            [whole((HEAD, ROWS))] * 2 + [whole((NZ, KVG, ROWS))],
            (whole((ROWS, 128)),) * 2,
            (q_all[turns[0]], q_all[turns[1]], kvg),
            scratch=[pltpu.VMEM((NZ, DEPTH, ROWS), BF16)],
            flops=10_000_000_000,
        )

    def send_part(part, d):
        return lax.ppermute(part, "x", [(i, (i + d) % NX) for i in range(NX)])

    part1, part2 = attend((1, 2))
    part1, part2 = send_part(part1, 1), send_part(part2, 2)

    part3, part0 = attend((3, 0))
    part3 = send_part(part3, 3)

    rows, shared = call(
        sum_body,
        (
            jax.ShapeDtypeStruct((2 * SLOTS, 128), BF16),
            jax.ShapeDtypeStruct((64, 256), F32),
        ),
        ids,
        (1,),
        [whole((NY, SLOTS + 64, 256)), whole((2 * SLOTS, 8))],
        (whole((2 * SLOTS, 128)), whole((64, 256))),
        (products, table),
        flops=1_000_000_000,
    )
    returned = lax.all_to_all(rows, ("z", "x"), 0, 0, tiled=True)

    mixed = call(
        combine_body,
        jax.ShapeDtypeStruct((HEAD, ROWS), BF16),
        ids,
        (1,),
        [whole((1, HEAD))] + [whole((ROWS, 128))] * NX,
        whole((HEAD, ROWS)),
        (head_gain.reshape(1, HEAD), part0, part1, part2, part3),
    ).T

    own, give = call(
        weigh_body,
        (jax.ShapeDtypeStruct((TOK, 128), F32), jax.ShapeDtypeStruct((TOK, 128), F32)),
        ids,
        (1,),
        [
            whole((2 * SLOTS, 128)),
            whole((TOK, 4)),
            whole((TOK, 4)),
            whole((8, 2 * SLOTS)),
            whole((64, 256)),
        ],
        (whole((TOK, 128)), whole((TOK, 128))),
        (returned, routes, route_weight, table.T, shared),
        flops=1_000_000_000,
    )
    taken = lax.ppermute(give, "c", swap)
    expert_out = (own + taken).astype(BF16)
    return (mixed, expert_out)


def solution(mesh):
    fine = Mesh(mesh.devices.reshape(NZ, NX, NY, NC), ("z", "x", "y", "c"))
    ep, tp = ("z", "x"), ("y", "c")
    in_specs = (
        P(ep, tp),
        P(ep, tp),
        P(ep, tp),
        P(ep, tp),
        P(tp),
        P(ep, None),
        P(),
        P(ep, None),
        P(ep, None),
        P(ep, tp, None),
        P(ep, tp, None),
        P(ep, tp, None),
        P(tp, None),
        P(tp, None),
        P(tp, None),
    )
    out_specs = (P(ep, tp), P(ep, tp))

    return jax.shard_map(
        on_device, mesh=fine, in_specs=in_specs, out_specs=out_specs, check_vma=False
    )
```

```python
import functools

import jax
import jax.numpy as jnp
import numpy as np
from jax import lax
from jax.experimental import pallas as pl
from jax.experimental.pallas import tpu as pltpu
from jax.sharding import Mesh
from jax.sharding import PartitionSpec as P


NORM_EPSILON = 1e-06
LOG2E = 1.4426950408889634
NEG = -1e30
NZ, NX, NY, NC = 8, 4, 8, 2
N_EP = NZ * NX
ROWS = 768
HEAD = 64
D = 2048
TOK = 128
CAP = 6
LOCAL = 2
SLOTS = N_EP * LOCAL * CAP
KG = HEAD + 16
KVG = KG + HEAD
F32 = jnp.float32
BF16 = jnp.bfloat16


def wide_slots():
    s = np.arange(2 * SLOTS)
    e, h, j = s // 24, (s % 24) // 12, s % 12
    return e, h, j // CAP, j % CAP


def slot_table():
    e, h, l, p = wide_slots()
    table = np.zeros((2 * SLOTS, 8), np.int32)
    table[:, 0] = 4 * e + l
    table[:, 1] = p
    table[:, 2] = h
    table[:, 3] = l * (SLOTS // 2) + e * CAP + p
    return table


def source_table():
    r = np.arange(SLOTS)
    l, e, p = r // (SLOTS // 2), (r % (SLOTS // 2)) // CAP, r % CAP
    table = np.zeros((SLOTS, 8), np.int32)
    table[:, 0] = e * 24 + l * CAP + p
    table[:, 1] = table[:, 0] + 12
    return table


def dot(a, b):
    return jnp.dot(a, b, preferred_element_type=F32)


def dot_t(a, b):
    return lax.dot_general(a, b, (((1,), (1,)), ((), ())), preferred_element_type=F32)


def three_pieces(v):
    hi = v.astype(BF16)
    rest = v - hi.astype(F32)
    mid = rest.astype(BF16)
    lo = (rest - mid.astype(F32)).astype(BF16)
    return hi, mid, lo


def call(body, out_shape, scalars, grid, in_specs, out_specs, args, scratch=(), flops=0, aliases=None):
    return pl.pallas_call(
        body,
        out_shape=out_shape,
        grid_spec=pltpu.PrefetchScalarGridSpec(
            num_scalar_prefetch=1,
            grid=grid,
            in_specs=in_specs,
            out_specs=out_specs,
            scratch_shapes=list(scratch),
        ),
        compiler_params=pltpu.CompilerParams(
            dimension_semantics=("arbitrary",) * len(grid), vmem_limit_bytes=56 * 2**20
        ),
        input_output_aliases=aliases or {},
        cost_estimate=pl.CostEstimate(flops=flops, bytes_accessed=4 << 20, transcendentals=0),
    )(scalars, *args)


def whole(shape):
    return pl.BlockSpec(shape, lambda i, s: (0,) * len(shape))


UNREAD = pl.BlockSpec(memory_space=pl.ANY)


def pack_body(ids, k_ref, v_ref, g_ref, out_ref):
    out_ref[0:HEAD, :] = k_ref[...]
    out_ref[KG:KVG, :] = v_ref[...]
    hi, mid, lo = three_pieces(g_ref[...] * (-LOG2E))
    row = lax.broadcasted_iota(jnp.int32, (16, ROWS), 0)
    zero = jnp.zeros((16, ROWS), F32)
    pieces = jnp.where(
        row == 0,
        hi.astype(F32),
        jnp.where(row == 1, mid.astype(F32), jnp.where(row == 2, lo.astype(F32), zero)),
    )
    out_ref[HEAD:KG, :] = pieces.astype(BF16)


def trade_body(ids, gate_ref, up_ref, down_ref, sgate_ref, sup_ref, sdown_ref, after_ref, out_ref):
    for i, ref in enumerate((gate_ref, up_ref, down_ref)):
        for l in range(LOCAL):
            out_ref[i * 128 + l * 64 : i * 128 + l * 64 + 64, :] = ref[l]
    for i, ref in enumerate((sgate_ref, sup_ref, sdown_ref)):
        out_ref[384 + i * 32 : 416 + i * 32, :] = ref[...]


TILE = 384
TILES = ROWS // TILE
DEPTH = 2 * HEAD + 16


def attend_body(turns, ids, q0_ref, q1_ref, *refs):
    chunks, (out0_ref, out1_ref, ka_ref, v_ref) = refs[:NZ], refs[NZ:]
    z, x = ids[0], ids[1]
    for back, ref in enumerate(chunks):
        place = lax.rem(z + NZ - back, NZ)
        ka_ref[place, 0:HEAD, :] = ref[0:HEAD, :]
        ka_ref[place, HEAD:DEPTH, :] = ref[0:KG, :]
        v_ref[place] = ref[KG:KVG, :]
    tiles = []
    for ref in (q0_ref, q1_ref):
        scaled = ref[...].astype(F32).T * (0.125 * LOG2E)
        hi = scaled.astype(BF16)
        lo = (scaled - hi.astype(F32)).astype(BF16)
        rows = jnp.concatenate([hi, lo, jnp.ones((ROWS, 16), BF16)], axis=1)
        tiles += [rows[i * TILE : (i + 1) * TILE] for i in range(TILES)]

    def weigh(s, values, peak, acc):
        new_peak = jnp.maximum(peak, jnp.max(s, axis=1, keepdims=True))
        w = jnp.exp2(s - new_peak).astype(BF16)
        return new_peak, acc * jnp.exp2(peak - new_peak) + dot_t(w, values)

    def update(chunk, carry, some, masked):
        k, values = ka_ref[chunk], v_ref[chunk]
        scores = [dot(tile, k) for tile in some]
        if masked:
            for i in range(TILES):
                row = lax.broadcasted_iota(jnp.int32, (TILE, ROWS), 0) + i * TILE
                col = lax.broadcasted_iota(jnp.int32, (TILE, ROWS), 1)
                scores[i] = jnp.where(col <= row, scores[i], NEG)
        return tuple(weigh(s, values, *c) for s, c in zip(scores, carry))

    start = ((jnp.full((TILE, 1), NEG, F32), jnp.zeros((TILE, HEAD), F32)),) * (2 * TILES)
    carry = lax.fori_loop(0, z, lambda i, c: update(i, c, tiles, False), start)
    lane = lax.broadcasted_iota(jnp.int32, (ROWS, HEAD), 1)
    for n, (turn, ref) in enumerate(zip(turns, (out0_ref, out1_ref))):
        mine = slice(n * TILES, (n + 1) * TILES)
        if turn == 0:
            last = update(z, carry[mine], tiles[mine], True)
        else:
            last = lax.cond(
                lax.rem(x + turn, NX) > x,
                lambda c, some=tiles[mine]: update(z, c, some, False),
                lambda c: c,
                carry[mine],
            )
        acc = jnp.concatenate([c[1] for c in last], axis=0)
        p_hi, p_mid, p_lo = three_pieces(jnp.concatenate([c[0] for c in last], axis=0))
        tail = jnp.where(
            lane == 0,
            p_hi.astype(F32),
            jnp.where(
                lane == 1,
                p_mid.astype(F32),
                jnp.where(lane == 2, p_lo.astype(F32), jnp.zeros((), F32)),
            ),
        )
        ref[...] = jnp.concatenate([acc, tail], axis=1).astype(BF16)


def combine_body(ids, gain_ref, *refs):
    out_ref, parts = refs[-1], refs[:-1]
    peaks = []
    for ref in parts:
        tail = ref[:, HEAD : HEAD + 3].astype(F32)
        peaks.append(tail[:, 0:1] + tail[:, 1:2] + tail[:, 2:3])
    top = jnp.maximum(jnp.maximum(peaks[0], peaks[1]), jnp.maximum(peaks[2], peaks[3]))
    total = jnp.zeros((ROWS, HEAD), F32)
    for ref, peak in zip(parts, peaks):
        total = total + ref[:, 0:HEAD].astype(F32) * jnp.exp2(peak - top)
    mean_square = jnp.mean(total * total, axis=1, keepdims=True)
    out = total * lax.rsqrt(mean_square + NORM_EPSILON) * gain_ref[...]
    out_ref[...] = out.T.astype(BF16)


def dispatch_body(ids, x_ref, gain_ref, routes_ref, table_ref, after_ref, normed_ref, send_ref):
    c = ids[2]
    x = x_ref[...].astype(F32)
    mean_square = jnp.mean(x * x, axis=1, keepdims=True)
    normed = (x * lax.rsqrt(mean_square + NORM_EPSILON) * gain_ref[...]).astype(BF16)
    normed_ref[...] = normed
    expert = table_ref[:, 0:1] + 2 * c
    member = jnp.zeros((2 * SLOTS, TOK), F32)
    for k in range(4):
        member = jnp.where(routes_ref[k : k + 1, :] == expert, 1.0, member)
    before = lax.broadcasted_iota(jnp.int32, (TOK, TOK), 0)
    after = lax.broadcasted_iota(jnp.int32, (TOK, TOK), 1)
    earlier = jnp.where(before < after, 1.0, 0.0).astype(BF16)
    rank = dot(member.astype(BF16), earlier)
    pick = jnp.where(rank == table_ref[:, 1:2].astype(F32), member, 0.0)
    half = table_ref[:, 2:3]
    first = jnp.where(half == 0, pick, 0.0).astype(BF16)
    second = jnp.where(half == 1, pick, 0.0).astype(BF16)
    at = lax.rem(ids[3], 2) * (D // 2)
    low = normed_ref[:, pl.ds(pl.multiple_of(at, D // 2), D // 4)]
    high = normed_ref[:, pl.ds(pl.multiple_of(at + D // 4, D // 4), D // 4)]
    send_ref[...] = (dot(first, low) + dot(second, high)).astype(BF16)


def gated(g, u):
    return g / (1.0 + jnp.exp(-g)) * u


def experts_body(
    ids,
    x_ref,
    x_got_ref,
    gate_ref,
    up_ref,
    down_ref,
    got_ref,
    normed_ref,
    sgate_ref,
    sup_ref,
    sdown_ref,
    source_ref,
    out_ref,
    low_ref,
    high_ref,
):
    c = ids[2]
    even = lax.rem(ids[3], 2) == 0

    @pl.when(even)
    def _():
        low_ref[...] = x_ref[...]
        high_ref[...] = x_got_ref[...]

    @pl.when(jnp.logical_not(even))
    def _():
        low_ref[...] = x_got_ref[...]
        high_ref[...] = x_ref[...]

    lane = lax.broadcasted_iota(jnp.int32, (SLOTS, 2 * SLOTS), 1)
    x0 = jnp.where(lane == source_ref[:, 0:1], 1.0, 0.0).astype(BF16)
    x1 = jnp.where(lane == source_ref[:, 1:2], 1.0, 0.0).astype(BF16)
    low, high = low_ref[...], high_ref[...]
    rows = jnp.concatenate([dot(x0, low), dot(x1, low), dot(x0, high), dot(x1, high)], axis=1)
    rows = rows.astype(BF16)
    n = SLOTS // 2
    for l in range(LOCAL):
        wg = jnp.concatenate([gate_ref[l], got_ref[l * 64 : l * 64 + 64, :]], axis=0)
        wu = jnp.concatenate([up_ref[l], got_ref[128 + l * 64 : 128 + l * 64 + 64, :]], axis=0)
        g, u = dot_t(rows[l * n : (l + 1) * n], wg), dot_t(rows[l * n : (l + 1) * n], wu)
        h = gated(g, u).astype(BF16)
        wd = jnp.concatenate([down_ref[l], got_ref[256 + l * 64 : 320 + l * 64, :]], axis=0)
        for y in range(NY):
            out_ref[y, l * n : (l + 1) * n, :] = dot(h, wd[:, y * 256 : y * 256 + 256]).astype(BF16)
    tokens = normed_ref[pl.ds(pl.multiple_of(c * 64, 64), 64), :]
    wg = jnp.concatenate([sgate_ref[...], got_ref[384:416, :]], axis=0)
    wu = jnp.concatenate([sup_ref[...], got_ref[416:448, :]], axis=0)
    h = gated(dot_t(tokens, wg), dot_t(tokens, wu)).astype(BF16)
    wd = jnp.concatenate([sdown_ref[...], got_ref[448:480, :]], axis=0)
    for y in range(NY):
        part = dot(h, wd[:, y * 256 : y * 256 + 256])
        out_ref[y, SLOTS : SLOTS + 64, :] = part.astype(BF16)


def sum_body(ids, part_ref, table_ref, out_ref, shared_ref):
    total = jnp.zeros((SLOTS + 64, 256), F32)
    for y in range(NY):
        total = total + part_ref[y].astype(F32)
    shared_ref[...] = total[SLOTS:]
    rows = total[:SLOTS].astype(BF16)
    lane = lax.broadcasted_iota(jnp.int32, (2 * SLOTS, SLOTS), 1)
    place = jnp.where(lane == table_ref[:, 3:4], 1.0, 0.0)
    half = table_ref[:, 2:3]
    first = jnp.where(half == 0, place, 0.0).astype(BF16)
    second = jnp.where(half == 1, place, 0.0).astype(BF16)
    out_ref[...] = (dot(first, rows[:, :128]) + dot(second, rows[:, 128:])).astype(BF16)


def weigh_body(ids, y_ref, routes_ref, weight_ref, table_ref, shared_ref, own_ref, send_ref):
    c = ids[2]
    expert = table_ref[0:1, :] + 2 * c
    member = jnp.zeros((TOK, 2 * SLOTS), F32)
    weight = jnp.zeros((TOK, 2 * SLOTS), F32)
    for k in range(4):
        same = routes_ref[:, k : k + 1] == expert
        member = jnp.where(same, 1.0, member)
        weight = jnp.where(same, weight_ref[:, k : k + 1], weight)
    after = lax.broadcasted_iota(jnp.int32, (TOK, TOK), 0)
    before = lax.broadcasted_iota(jnp.int32, (TOK, TOK), 1)
    earlier = jnp.where(before < after, 1.0, 0.0).astype(BF16)
    rank = dot(earlier, member.astype(BF16))
    weight = jnp.where(rank == table_ref[1:2, :].astype(F32), weight, 0.0)
    half = table_ref[2:3, :]
    y = y_ref[...]
    row = lax.broadcasted_iota(jnp.int32, (TOK, 128), 0)
    mine = (row >= c * 64) & (row < c * 64 + 64)
    shared = shared_ref[...]
    shared = jnp.concatenate([shared, shared], axis=0)
    for which, ref in ((c, own_ref), (1 - c, send_ref)):
        part = jnp.where(half == which, weight, 0.0)
        total = jnp.zeros((TOK, 128), F32)
        for piece in three_pieces(part):
            total = total + dot(piece, y)
        columns = jnp.where(which == 0, shared[:, :128], shared[:, 128:])
        ref[...] = total + jnp.where(mine, columns, 0.0)


def on_device(
    queries,
    keys,
    values,
    cum_gate,
    head_gain,
    moe_in,
    ffn_gain,
    routes,
    route_weight,
    expert_gate,
    expert_up,
    expert_down,
    shared_gate,
    shared_up,
    shared_down,
):
    z, x, y, c = (lax.axis_index(a) for a in ("z", "x", "y", "c"))
    ids = jnp.stack([z, x, c, y]).astype(jnp.int32)
    table = jnp.asarray(slot_table())
    source = jnp.asarray(source_table())
    swap = [(0, 1), (1, 0)]

    packed = call(
        pack_body,
        jax.ShapeDtypeStruct((KVG, ROWS), BF16),
        ids,
        (1,),
        [whole((HEAD, ROWS)), whole((HEAD, ROWS)), whole((1, ROWS))],
        whole((KVG, ROWS)),
        (keys.T, values.T, cum_gate.reshape(1, ROWS)),
    )
    later = [(i, (i + 1) % NZ) for i in range(NZ)]
    earlier = [(i, (i - 1) % NZ) for i in range(NZ)]
    rising, falling = [packed], [packed]
    for turn in range(1, 5):
        rising.append(lax.ppermute(rising[-1], "z", later))
        if turn < 4:
            falling.append(lax.ppermute(falling[-1], "z", earlier))
    kvg = rising + falling[:0:-1]

    normed, sent = call(
        dispatch_body,
        (
            jax.ShapeDtypeStruct((TOK, D), BF16),
            jax.ShapeDtypeStruct((2 * SLOTS, D // 4), BF16),
        ),
        ids,
        (1,),
        [whole((TOK, D)), whole((1, D)), whole((4, TOK)), whole((2 * SLOTS, 8)), UNREAD],
        (whole((TOK, D)), whole((2 * SLOTS, D // 4))),
        (moe_in, ffn_gain.reshape(1, D), routes.T, table, packed),
        flops=1_000_000_000,
    )
    arrived = lax.all_to_all(sent, ("z", "x"), 0, 0, tiled=True)
    arrived_too = lax.ppermute(arrived, "y", [(i, i ^ 1) for i in range(NY)])

    other = pl.BlockSpec((LOCAL, 64, D), lambda i, s: (1 - s[2], 0, 0))
    trade = call(
        trade_body,
        jax.ShapeDtypeStruct((480, D), BF16),
        ids,
        (1,),
        [other, other, other, whole((32, D)), whole((32, D)), whole((32, D)), UNREAD],
        whole((480, D)),
        (expert_gate, expert_up, expert_down, shared_gate, shared_up, shared_down, sent),
        flops=1_000_000_000,
    )
    got = lax.ppermute(trade, "c", swap)

    mine, _ = lax.optimization_barrier((queries.T, trade))
    q_all = [mine] + [
        lax.ppermute(mine, "x", [((i + d) % NX, i) for i in range(NX)]) for d in range(1, NX)
    ]

    mine = pl.BlockSpec((LOCAL, 64, D), lambda i, s: (s[2], 0, 0))
    products = call(
        experts_body,
        jax.ShapeDtypeStruct((NY, SLOTS + 64, 256), BF16),
        ids,
        (1,),
        [
            whole((2 * SLOTS, D // 4)),
            whole((2 * SLOTS, D // 4)),
            mine,
            mine,
            mine,
            whole((480, D)),
            whole((TOK, D)),
            whole((32, D)),
            whole((32, D)),
            whole((32, D)),
            whole((SLOTS, 8)),
        ],
        whole((NY, SLOTS + 64, 256)),
        (
            arrived,
            arrived_too,
            expert_gate,
            expert_up,
            expert_down,
            got,
            normed,
            shared_gate,
            shared_up,
            shared_down,
            source,
        ),
        scratch=[pltpu.VMEM((2 * SLOTS, D // 4), BF16)] * 2,
        flops=1_000_000_000,
    )
    products = lax.all_to_all(products, "y", 0, 0, tiled=True)

    def attend(turns):
        return call(
            functools.partial(attend_body, turns),
            (jax.ShapeDtypeStruct((ROWS, 128), BF16),) * 2,
            ids,
            (1,),
            [whole((HEAD, ROWS))] * 2 + [whole((KVG, ROWS))] * NZ,
            (whole((ROWS, 128)),) * 2,
            (q_all[turns[0]], q_all[turns[1]], *kvg),
            scratch=[pltpu.VMEM((NZ, DEPTH, ROWS), BF16), pltpu.VMEM((NZ, HEAD, ROWS), BF16)],
            flops=10_000_000_000,
        )

    def send_part(part, d):
        return lax.ppermute(part, "x", [(i, (i + d) % NX) for i in range(NX)])

    part1, part2 = attend((1, 2))
    part1, part2 = send_part(part1, 1), send_part(part2, 2)

    part3, part0 = attend((3, 0))
    part3 = send_part(part3, 3)

    rows, shared = call(
        sum_body,
        (
            jax.ShapeDtypeStruct((2 * SLOTS, 128), BF16),
            jax.ShapeDtypeStruct((64, 256), F32),
        ),
        ids,
        (1,),
        [whole((NY, SLOTS + 64, 256)), whole((2 * SLOTS, 8))],
        (whole((2 * SLOTS, 128)), whole((64, 256))),
        (products, table),
        flops=1_000_000_000,
    )
    returned = lax.all_to_all(rows, ("z", "x"), 0, 0, tiled=True)

    mixed = call(
        combine_body,
        jax.ShapeDtypeStruct((HEAD, ROWS), BF16),
        ids,
        (1,),
        [whole((1, HEAD))] + [whole((ROWS, 128))] * NX,
        whole((HEAD, ROWS)),
        (head_gain.reshape(1, HEAD), part0, part1, part2, part3),
    ).T

    own, give = call(
        weigh_body,
        (jax.ShapeDtypeStruct((TOK, 128), F32), jax.ShapeDtypeStruct((TOK, 128), F32)),
        ids,
        (1,),
        [
            whole((2 * SLOTS, 128)),
            whole((TOK, 4)),
            whole((TOK, 4)),
            whole((8, 2 * SLOTS)),
            whole((64, 256)),
        ],
        (whole((TOK, 128)), whole((TOK, 128))),
        (returned, routes, route_weight, table.T, shared),
        flops=1_000_000_000,
    )
    taken = lax.ppermute(give, "c", swap)
    expert_out = (own + taken).astype(BF16)
    return (mixed, expert_out)


def solution(mesh):
    fine = Mesh(mesh.devices.reshape(NZ, NX, NY, NC), ("z", "x", "y", "c"))
    ep, tp = ("z", "x"), ("y", "c")
    in_specs = (
        P(ep, tp),
        P(ep, tp),
        P(ep, tp),
        P(ep, tp),
        P(tp),
        P(ep, None),
        P(),
        P(ep, None),
        P(ep, None),
        P(ep, tp, None),
        P(ep, tp, None),
        P(ep, tp, None),
        P(tp, None),
        P(tp, None),
        P(tp, None),
    )
    out_specs = (P(ep, tp), P(ep, tp))

    return jax.shard_map(
        on_device, mesh=fine, in_specs=in_specs, out_specs=out_specs, check_vma=False
    )
```

```python
import functools

import jax
import jax.numpy as jnp
import numpy as np
from jax import lax
from jax.experimental import pallas as pl
from jax.experimental.pallas import tpu as pltpu
from jax.sharding import Mesh
from jax.sharding import PartitionSpec as P


NORM_EPSILON = 1e-06
LOG2E = 1.4426950408889634
NEG = -1e30
NZ, NX, NY, NC = 8, 4, 8, 2
N_EP = NZ * NX
ROWS = 768
HEAD = 64
D = 2048
TOK = 128
CAP = 6
LOCAL = 2
SLOTS = N_EP * LOCAL * CAP
KG = HEAD + 16
KVG = KG + HEAD
F32 = jnp.float32
BF16 = jnp.bfloat16


def wide_slots():
    s = np.arange(2 * SLOTS)
    e, h, j = s // 24, (s % 24) // 12, s % 12
    return e, h, j // CAP, j % CAP


def slot_table():
    e, h, l, p = wide_slots()
    table = np.zeros((2 * SLOTS, 8), np.int32)
    table[:, 0] = 4 * e + l
    table[:, 1] = p
    table[:, 2] = h
    table[:, 3] = l * (SLOTS // 2) + e * CAP + p
    return table


def source_table():
    r = np.arange(SLOTS)
    l, e, p = r // (SLOTS // 2), (r % (SLOTS // 2)) // CAP, r % CAP
    table = np.zeros((SLOTS, 8), np.int32)
    table[:, 0] = e * 24 + l * CAP + p
    table[:, 1] = table[:, 0] + 12
    return table


def dot(a, b):
    return jnp.dot(a, b, preferred_element_type=F32)


def dot_t(a, b):
    return lax.dot_general(a, b, (((1,), (1,)), ((), ())), preferred_element_type=F32)


def three_pieces(v):
    hi = v.astype(BF16)
    rest = v - hi.astype(F32)
    mid = rest.astype(BF16)
    lo = (rest - mid.astype(F32)).astype(BF16)
    return hi, mid, lo


def call(body, out_shape, scalars, grid, in_specs, out_specs, args, scratch=(), flops=0, aliases=None):
    return pl.pallas_call(
        body,
        out_shape=out_shape,
        grid_spec=pltpu.PrefetchScalarGridSpec(
            num_scalar_prefetch=1,
            grid=grid,
            in_specs=in_specs,
            out_specs=out_specs,
            scratch_shapes=list(scratch),
        ),
        compiler_params=pltpu.CompilerParams(
            dimension_semantics=("arbitrary",) * len(grid), vmem_limit_bytes=56 * 2**20
        ),
        input_output_aliases=aliases or {},
        cost_estimate=pl.CostEstimate(flops=flops, bytes_accessed=4 << 20, transcendentals=0),
    )(scalars, *args)


def whole(shape):
    return pl.BlockSpec(shape, lambda i, s: (0,) * len(shape))


UNREAD = pl.BlockSpec(memory_space=pl.ANY)


def pack_body(ids, k_ref, v_ref, g_ref, after_ref, out_ref):
    out_ref[0:HEAD, :] = k_ref[...]
    out_ref[KG:KVG, :] = v_ref[...]
    hi, mid, lo = three_pieces(g_ref[...] * (-LOG2E))
    row = lax.broadcasted_iota(jnp.int32, (16, ROWS), 0)
    zero = jnp.zeros((16, ROWS), F32)
    pieces = jnp.where(
        row == 0,
        hi.astype(F32),
        jnp.where(row == 1, mid.astype(F32), jnp.where(row == 2, lo.astype(F32), zero)),
    )
    out_ref[HEAD:KG, :] = pieces.astype(BF16)


def trade_body(ids, gate_ref, up_ref, down_ref, sgate_ref, sup_ref, sdown_ref, after_ref, out_ref):
    for i, ref in enumerate((gate_ref, up_ref, down_ref)):
        for l in range(LOCAL):
            out_ref[i * 128 + l * 64 : i * 128 + l * 64 + 64, :] = ref[l]
    for i, ref in enumerate((sgate_ref, sup_ref, sdown_ref)):
        out_ref[384 + i * 32 : 416 + i * 32, :] = ref[...]


TILE = 384
TILES = ROWS // TILE
DEPTH = 2 * HEAD + 16


def attend_body(turns, ids, q0_ref, q1_ref, *refs):
    chunks, (out0_ref, out1_ref, ka_ref, v_ref) = refs[:NZ], refs[NZ:]
    z, x = ids[0], ids[1]
    for back, ref in enumerate(chunks):
        place = lax.rem(z + NZ - back, NZ)
        ka_ref[place, 0:HEAD, :] = ref[0:HEAD, :]
        ka_ref[place, HEAD:DEPTH, :] = ref[0:KG, :]
        v_ref[place] = ref[KG:KVG, :]
    tiles = []
    for ref in (q0_ref, q1_ref):
        scaled = ref[...].astype(F32).T * (0.125 * LOG2E)
        hi = scaled.astype(BF16)
        lo = (scaled - hi.astype(F32)).astype(BF16)
        rows = jnp.concatenate([hi, lo, jnp.ones((ROWS, 16), BF16)], axis=1)
        tiles += [rows[i * TILE : (i + 1) * TILE] for i in range(TILES)]

    def weigh(s, values, peak, acc):
        new_peak = jnp.maximum(peak, jnp.max(s, axis=1, keepdims=True))
        w = jnp.exp2(s - new_peak).astype(BF16)
        return new_peak, acc * jnp.exp2(peak - new_peak) + dot_t(w, values)

    def update(chunk, carry, some, masked):
        k, values = ka_ref[chunk], v_ref[chunk]
        scores = [dot(tile, k) for tile in some]
        if masked:
            for i in range(TILES):
                row = lax.broadcasted_iota(jnp.int32, (TILE, ROWS), 0) + i * TILE
                col = lax.broadcasted_iota(jnp.int32, (TILE, ROWS), 1)
                scores[i] = jnp.where(col <= row, scores[i], NEG)
        return tuple(weigh(s, values, *c) for s, c in zip(scores, carry))

    start = ((jnp.full((TILE, 1), NEG, F32), jnp.zeros((TILE, HEAD), F32)),) * (2 * TILES)
    carry = lax.fori_loop(0, z, lambda i, c: update(i, c, tiles, False), start)
    lane = lax.broadcasted_iota(jnp.int32, (ROWS, HEAD), 1)
    for n, (turn, ref) in enumerate(zip(turns, (out0_ref, out1_ref))):
        mine = slice(n * TILES, (n + 1) * TILES)
        if turn == 0:
            last = update(z, carry[mine], tiles[mine], True)
        else:
            last = lax.cond(
                lax.rem(x + turn, NX) > x,
                lambda c, some=tiles[mine]: update(z, c, some, False),
                lambda c: c,
                carry[mine],
            )
        acc = jnp.concatenate([c[1] for c in last], axis=0)
        p_hi, p_mid, p_lo = three_pieces(jnp.concatenate([c[0] for c in last], axis=0))
        tail = jnp.where(
            lane == 0,
            p_hi.astype(F32),
            jnp.where(
                lane == 1,
                p_mid.astype(F32),
                jnp.where(lane == 2, p_lo.astype(F32), jnp.zeros((), F32)),
            ),
        )
        ref[...] = jnp.concatenate([acc, tail], axis=1).astype(BF16)


def combine_body(ids, gain_ref, *refs):
    out_ref, parts = refs[-1], refs[:-1]
    peaks = []
    for ref in parts:
        tail = ref[:, HEAD : HEAD + 3].astype(F32)
        peaks.append(tail[:, 0:1] + tail[:, 1:2] + tail[:, 2:3])
    top = jnp.maximum(jnp.maximum(peaks[0], peaks[1]), jnp.maximum(peaks[2], peaks[3]))
    total = jnp.zeros((ROWS, HEAD), F32)
    for ref, peak in zip(parts, peaks):
        total = total + ref[:, 0:HEAD].astype(F32) * jnp.exp2(peak - top)
    mean_square = jnp.mean(total * total, axis=1, keepdims=True)
    out = total * lax.rsqrt(mean_square + NORM_EPSILON) * gain_ref[...]
    out_ref[...] = out.T.astype(BF16)


def dispatch_body(ids, x_ref, gain_ref, routes_ref, table_ref, normed_ref, send_ref):
    c = ids[2]
    x = x_ref[...].astype(F32)
    mean_square = jnp.mean(x * x, axis=1, keepdims=True)
    normed = (x * lax.rsqrt(mean_square + NORM_EPSILON) * gain_ref[...]).astype(BF16)
    normed_ref[...] = normed
    expert = table_ref[:, 0:1] + 2 * c
    member = jnp.zeros((2 * SLOTS, TOK), F32)
    for k in range(4):
        member = jnp.where(routes_ref[k : k + 1, :] == expert, 1.0, member)
    before = lax.broadcasted_iota(jnp.int32, (TOK, TOK), 0)
    after = lax.broadcasted_iota(jnp.int32, (TOK, TOK), 1)
    earlier = jnp.where(before < after, 1.0, 0.0).astype(BF16)
    rank = dot(member.astype(BF16), earlier)
    pick = jnp.where(rank == table_ref[:, 1:2].astype(F32), member, 0.0)
    half = table_ref[:, 2:3]
    first = jnp.where(half == 0, pick, 0.0).astype(BF16)
    second = jnp.where(half == 1, pick, 0.0).astype(BF16)
    at = lax.rem(ids[3], 2) * (D // 2)
    low = normed_ref[:, pl.ds(pl.multiple_of(at, D // 2), D // 4)]
    high = normed_ref[:, pl.ds(pl.multiple_of(at + D // 4, D // 4), D // 4)]
    send_ref[...] = (dot(first, low) + dot(second, high)).astype(BF16)


def gated(g, u):
    return g / (1.0 + jnp.exp(-g)) * u


def experts_body(
    ids,
    x_ref,
    x_got_ref,
    gate_ref,
    up_ref,
    down_ref,
    got_ref,
    normed_ref,
    sgate_ref,
    sup_ref,
    sdown_ref,
    source_ref,
    out_ref,
    low_ref,
    high_ref,
):
    c = ids[2]
    even = lax.rem(ids[3], 2) == 0

    @pl.when(even)
    def _():
        low_ref[...] = x_ref[...]
        high_ref[...] = x_got_ref[...]

    @pl.when(jnp.logical_not(even))
    def _():
        low_ref[...] = x_got_ref[...]
        high_ref[...] = x_ref[...]

    lane = lax.broadcasted_iota(jnp.int32, (SLOTS, 2 * SLOTS), 1)
    x0 = jnp.where(lane == source_ref[:, 0:1], 1.0, 0.0).astype(BF16)
    x1 = jnp.where(lane == source_ref[:, 1:2], 1.0, 0.0).astype(BF16)
    low, high = low_ref[...], high_ref[...]
    rows = jnp.concatenate([dot(x0, low), dot(x1, low), dot(x0, high), dot(x1, high)], axis=1)
    rows = rows.astype(BF16)
    n = SLOTS // 2
    for l in range(LOCAL):
        wg = jnp.concatenate([gate_ref[l], got_ref[l * 64 : l * 64 + 64, :]], axis=0)
        wu = jnp.concatenate([up_ref[l], got_ref[128 + l * 64 : 128 + l * 64 + 64, :]], axis=0)
        g, u = dot_t(rows[l * n : (l + 1) * n], wg), dot_t(rows[l * n : (l + 1) * n], wu)
        h = gated(g, u).astype(BF16)
        wd = jnp.concatenate([down_ref[l], got_ref[256 + l * 64 : 320 + l * 64, :]], axis=0)
        for y in range(NY):
            out_ref[y, l * n : (l + 1) * n, :] = dot(h, wd[:, y * 256 : y * 256 + 256]).astype(BF16)
    tokens = normed_ref[pl.ds(pl.multiple_of(c * 64, 64), 64), :]
    wg = jnp.concatenate([sgate_ref[...], got_ref[384:416, :]], axis=0)
    wu = jnp.concatenate([sup_ref[...], got_ref[416:448, :]], axis=0)
    h = gated(dot_t(tokens, wg), dot_t(tokens, wu)).astype(BF16)
    wd = jnp.concatenate([sdown_ref[...], got_ref[448:480, :]], axis=0)
    for y in range(NY):
        part = dot(h, wd[:, y * 256 : y * 256 + 256])
        out_ref[y, SLOTS : SLOTS + 64, :] = part.astype(BF16)


def sum_body(ids, part_ref, table_ref, out_ref, shared_ref):
    total = jnp.zeros((SLOTS + 64, 256), F32)
    for y in range(NY):
        total = total + part_ref[y].astype(F32)
    shared_ref[...] = total[SLOTS:]
    rows = total[:SLOTS].astype(BF16)
    lane = lax.broadcasted_iota(jnp.int32, (2 * SLOTS, SLOTS), 1)
    place = jnp.where(lane == table_ref[:, 3:4], 1.0, 0.0)
    half = table_ref[:, 2:3]
    first = jnp.where(half == 0, place, 0.0).astype(BF16)
    second = jnp.where(half == 1, place, 0.0).astype(BF16)
    out_ref[...] = (dot(first, rows[:, :128]) + dot(second, rows[:, 128:])).astype(BF16)


def weigh_body(ids, y_ref, routes_ref, weight_ref, table_ref, shared_ref, own_ref, send_ref):
    c = ids[2]
    expert = table_ref[0:1, :] + 2 * c
    member = jnp.zeros((TOK, 2 * SLOTS), F32)
    weight = jnp.zeros((TOK, 2 * SLOTS), F32)
    for k in range(4):
        same = routes_ref[:, k : k + 1] == expert
        member = jnp.where(same, 1.0, member)
        weight = jnp.where(same, weight_ref[:, k : k + 1], weight)
    after = lax.broadcasted_iota(jnp.int32, (TOK, TOK), 0)
    before = lax.broadcasted_iota(jnp.int32, (TOK, TOK), 1)
    earlier = jnp.where(before < after, 1.0, 0.0).astype(BF16)
    rank = dot(earlier, member.astype(BF16))
    weight = jnp.where(rank == table_ref[1:2, :].astype(F32), weight, 0.0)
    half = table_ref[2:3, :]
    y = y_ref[...]
    row = lax.broadcasted_iota(jnp.int32, (TOK, 128), 0)
    mine = (row >= c * 64) & (row < c * 64 + 64)
    shared = shared_ref[...]
    shared = jnp.concatenate([shared, shared], axis=0)
    for which, ref in ((c, own_ref), (1 - c, send_ref)):
        part = jnp.where(half == which, weight, 0.0)
        total = jnp.zeros((TOK, 128), F32)
        for piece in three_pieces(part):
            total = total + dot(piece, y)
        columns = jnp.where(which == 0, shared[:, :128], shared[:, 128:])
        ref[...] = total + jnp.where(mine, columns, 0.0)


def on_device(
    queries,
    keys,
    values,
    cum_gate,
    head_gain,
    moe_in,
    ffn_gain,
    routes,
    route_weight,
    expert_gate,
    expert_up,
    expert_down,
    shared_gate,
    shared_up,
    shared_down,
):
    z, x, y, c = (lax.axis_index(a) for a in ("z", "x", "y", "c"))
    ids = jnp.stack([z, x, c, y]).astype(jnp.int32)
    table = jnp.asarray(slot_table())
    source = jnp.asarray(source_table())
    swap = [(0, 1), (1, 0)]

    normed, sent = call(
        dispatch_body,
        (
            jax.ShapeDtypeStruct((TOK, D), BF16),
            jax.ShapeDtypeStruct((2 * SLOTS, D // 4), BF16),
        ),
        ids,
        (1,),
        [whole((TOK, D)), whole((1, D)), whole((4, TOK)), whole((2 * SLOTS, 8))],
        (whole((TOK, D)), whole((2 * SLOTS, D // 4))),
        (moe_in, ffn_gain.reshape(1, D), routes.T, table),
        flops=1_000_000_000,
    )
    arrived = lax.all_to_all(sent, ("z", "x"), 0, 0, tiled=True)
    arrived_too = lax.ppermute(arrived, "y", [(i, i ^ 1) for i in range(NY)])

    packed = call(
        pack_body,
        jax.ShapeDtypeStruct((KVG, ROWS), BF16),
        ids,
        (1,),
        [whole((HEAD, ROWS)), whole((HEAD, ROWS)), whole((1, ROWS)), UNREAD],
        whole((KVG, ROWS)),
        (keys.T, values.T, cum_gate.reshape(1, ROWS), sent),
    )
    later = [(i, (i + 1) % NZ) for i in range(NZ)]
    earlier = [(i, (i - 1) % NZ) for i in range(NZ)]
    rising, falling = [packed], [packed]
    for turn in range(1, 5):
        rising.append(lax.ppermute(rising[-1], "z", later))
        if turn < 4:
            falling.append(lax.ppermute(falling[-1], "z", earlier))
    kvg = rising + falling[:0:-1]

    other = pl.BlockSpec((LOCAL, 64, D), lambda i, s: (1 - s[2], 0, 0))
    trade = call(
        trade_body,
        jax.ShapeDtypeStruct((480, D), BF16),
        ids,
        (1,),
        [other, other, other, whole((32, D)), whole((32, D)), whole((32, D)), UNREAD],
        whole((480, D)),
        (expert_gate, expert_up, expert_down, shared_gate, shared_up, shared_down, sent),
        flops=1_000_000_000,
    )
    got = lax.ppermute(trade, "c", swap)

    mine, _ = lax.optimization_barrier((queries.T, trade))
    q_all = [mine]
    for d in range(1, NX):
        q_all.append(lax.ppermute(mine, "x", [((i + d) % NX, i) for i in range(NX)]))

    mine = pl.BlockSpec((LOCAL, 64, D), lambda i, s: (s[2], 0, 0))
    products = call(
        experts_body,
        jax.ShapeDtypeStruct((NY, SLOTS + 64, 256), BF16),
        ids,
        (1,),
        [
            whole((2 * SLOTS, D // 4)),
            whole((2 * SLOTS, D // 4)),
            mine,
            mine,
            mine,
            whole((480, D)),
            whole((TOK, D)),
            whole((32, D)),
            whole((32, D)),
            whole((32, D)),
            whole((SLOTS, 8)),
        ],
        whole((NY, SLOTS + 64, 256)),
        (
            arrived,
            arrived_too,
            expert_gate,
            expert_up,
            expert_down,
            got,
            normed,
            shared_gate,
            shared_up,
            shared_down,
            source,
        ),
        scratch=[pltpu.VMEM((2 * SLOTS, D // 4), BF16)] * 2,
        flops=1_000_000_000,
    )
    products = lax.all_to_all(products, "y", 0, 0, tiled=True)

    def attend(turns):
        return call(
            functools.partial(attend_body, turns),
            (jax.ShapeDtypeStruct((ROWS, 128), BF16),) * 2,
            ids,
            (1,),
            [whole((HEAD, ROWS))] * 2 + [whole((KVG, ROWS))] * NZ,
            (whole((ROWS, 128)),) * 2,
            (q_all[turns[0]], q_all[turns[1]], *kvg),
            scratch=[pltpu.VMEM((NZ, DEPTH, ROWS), BF16), pltpu.VMEM((NZ, HEAD, ROWS), BF16)],
            flops=10_000_000_000,
        )

    def send_part(part, d):
        return lax.ppermute(part, "x", [(i, (i + d) % NX) for i in range(NX)])

    part1, part2 = attend((1, 2))
    part1, part2 = send_part(part1, 1), send_part(part2, 2)

    part3, part0 = attend((3, 0))
    part3 = send_part(part3, 3)

    rows, shared = call(
        sum_body,
        (
            jax.ShapeDtypeStruct((2 * SLOTS, 128), BF16),
            jax.ShapeDtypeStruct((64, 256), F32),
        ),
        ids,
        (1,),
        [whole((NY, SLOTS + 64, 256)), whole((2 * SLOTS, 8))],
        (whole((2 * SLOTS, 128)), whole((64, 256))),
        (products, table),
        flops=1_000_000_000,
    )
    returned = lax.all_to_all(rows, ("z", "x"), 0, 0, tiled=True)

    mixed = call(
        combine_body,
        jax.ShapeDtypeStruct((HEAD, ROWS), BF16),
        ids,
        (1,),
        [whole((1, HEAD))] + [whole((ROWS, 128))] * NX,
        whole((HEAD, ROWS)),
        (head_gain.reshape(1, HEAD), part0, part1, part2, part3),
    ).T

    own, give = call(
        weigh_body,
        (jax.ShapeDtypeStruct((TOK, 128), F32), jax.ShapeDtypeStruct((TOK, 128), F32)),
        ids,
        (1,),
        [
            whole((2 * SLOTS, 128)),
            whole((TOK, 4)),
            whole((TOK, 4)),
            whole((8, 2 * SLOTS)),
            whole((64, 256)),
        ],
        (whole((TOK, 128)), whole((TOK, 128))),
        (returned, routes, route_weight, table.T, shared),
        flops=1_000_000_000,
    )
    taken = lax.ppermute(give, "c", swap)
    expert_out = (own + taken).astype(BF16)
    return (mixed, expert_out)


def solution(mesh):
    fine = Mesh(mesh.devices.reshape(NZ, NX, NY, NC), ("z", "x", "y", "c"))
    ep, tp = ("z", "x"), ("y", "c")
    in_specs = (
        P(ep, tp),
        P(ep, tp),
        P(ep, tp),
        P(ep, tp),
        P(tp),
        P(ep, None),
        P(),
        P(ep, None),
        P(ep, None),
        P(ep, tp, None),
        P(ep, tp, None),
        P(ep, tp, None),
        P(tp, None),
        P(tp, None),
        P(tp, None),
    )
    out_specs = (P(ep, tp), P(ep, tp))

    return jax.shard_map(
        on_device, mesh=fine, in_specs=in_specs, out_specs=out_specs, check_vma=False
    )
```

```python
import functools

import jax
import jax.numpy as jnp
import numpy as np
from jax import lax
from jax.experimental import pallas as pl
from jax.experimental.pallas import tpu as pltpu
from jax.sharding import Mesh
from jax.sharding import PartitionSpec as P


NORM_EPSILON = 1e-06
LOG2E = 1.4426950408889634
NEG = -1e30
NZ, NX, NY, NC = 8, 4, 8, 2
N_EP = NZ * NX
ROWS = 768
HEAD = 64
D = 2048
TOK = 128
CAP = 6
LOCAL = 2
SLOTS = N_EP * LOCAL * CAP
KG = HEAD + 16
KVG = KG + HEAD
F32 = jnp.float32
BF16 = jnp.bfloat16


def wide_slots():
    s = np.arange(2 * SLOTS)
    e, h, j = s // 24, (s % 24) // 12, s % 12
    return e, h, j // CAP, j % CAP


def slot_table():
    e, h, l, p = wide_slots()
    table = np.zeros((2 * SLOTS, 8), np.int32)
    table[:, 0] = 4 * e + l
    table[:, 1] = p
    table[:, 2] = h
    table[:, 3] = l * (SLOTS // 2) + e * CAP + p
    return table


def source_table():
    r = np.arange(SLOTS)
    l, e, p = r // (SLOTS // 2), (r % (SLOTS // 2)) // CAP, r % CAP
    table = np.zeros((SLOTS, 8), np.int32)
    table[:, 0] = e * 24 + l * CAP + p
    table[:, 1] = table[:, 0] + 12
    return table


def dot(a, b):
    return jnp.dot(a, b, preferred_element_type=F32)


def dot_t(a, b):
    return lax.dot_general(a, b, (((1,), (1,)), ((), ())), preferred_element_type=F32)


def three_pieces(v):
    hi = v.astype(BF16)
    rest = v - hi.astype(F32)
    mid = rest.astype(BF16)
    lo = (rest - mid.astype(F32)).astype(BF16)
    return hi, mid, lo


def call(body, out_shape, scalars, grid, in_specs, out_specs, args, scratch=(), flops=0, aliases=None):
    return pl.pallas_call(
        body,
        out_shape=out_shape,
        grid_spec=pltpu.PrefetchScalarGridSpec(
            num_scalar_prefetch=1,
            grid=grid,
            in_specs=in_specs,
            out_specs=out_specs,
            scratch_shapes=list(scratch),
        ),
        compiler_params=pltpu.CompilerParams(
            dimension_semantics=("arbitrary",) * len(grid), vmem_limit_bytes=56 * 2**20
        ),
        input_output_aliases=aliases or {},
        cost_estimate=pl.CostEstimate(flops=flops, bytes_accessed=4 << 20, transcendentals=0),
    )(scalars, *args)


def whole(shape):
    return pl.BlockSpec(shape, lambda i, s: (0,) * len(shape))


UNREAD = pl.BlockSpec(memory_space=pl.ANY)


def pack_body(ids, k_ref, v_ref, g_ref, after_ref, out_ref):
    out_ref[0:HEAD, :] = k_ref[...]
    out_ref[KG:KVG, :] = v_ref[...]
    hi, mid, lo = three_pieces(g_ref[...] * (-LOG2E))
    row = lax.broadcasted_iota(jnp.int32, (16, ROWS), 0)
    zero = jnp.zeros((16, ROWS), F32)
    pieces = jnp.where(
        row == 0,
        hi.astype(F32),
        jnp.where(row == 1, mid.astype(F32), jnp.where(row == 2, lo.astype(F32), zero)),
    )
    out_ref[HEAD:KG, :] = pieces.astype(BF16)


def trade_body(ids, gate_ref, up_ref, down_ref, sgate_ref, sup_ref, sdown_ref, after_ref, out_ref):
    for i, ref in enumerate((gate_ref, up_ref, down_ref)):
        for l in range(LOCAL):
            out_ref[i * 128 + l * 64 : i * 128 + l * 64 + 64, :] = ref[l]
    for i, ref in enumerate((sgate_ref, sup_ref, sdown_ref)):
        out_ref[384 + i * 32 : 416 + i * 32, :] = ref[...]


TILE = 384
TILES = ROWS // TILE
DEPTH = 2 * HEAD + 16


def attend_body(turns, ids, q0_ref, q1_ref, *refs):
    chunks, (out0_ref, out1_ref, ka_ref, v_ref) = refs[:NZ], refs[NZ:]
    z, x = ids[0], ids[1]
    for back, ref in enumerate(chunks):
        place = lax.rem(z + NZ - back, NZ)
        ka_ref[place, 0:HEAD, :] = ref[0:HEAD, :]
        ka_ref[place, HEAD:DEPTH, :] = ref[0:KG, :]
        v_ref[place] = ref[KG:KVG, :]
    tiles = []
    for ref in (q0_ref, q1_ref):
        scaled = ref[...].astype(F32).T * (0.125 * LOG2E)
        hi = scaled.astype(BF16)
        lo = (scaled - hi.astype(F32)).astype(BF16)
        rows = jnp.concatenate([hi, lo, jnp.ones((ROWS, 16), BF16)], axis=1)
        tiles += [rows[i * TILE : (i + 1) * TILE] for i in range(TILES)]

    def weigh(s, values, peak, acc):
        new_peak = jnp.maximum(peak, jnp.max(s, axis=1, keepdims=True))
        w = jnp.exp2(s - new_peak).astype(BF16)
        return new_peak, acc * jnp.exp2(peak - new_peak) + dot_t(w, values)

    def update(chunk, carry, some, masked):
        k, values = ka_ref[chunk], v_ref[chunk]
        scores = [dot(tile, k) for tile in some]
        if masked:
            for i in range(TILES):
                row = lax.broadcasted_iota(jnp.int32, (TILE, ROWS), 0) + i * TILE
                col = lax.broadcasted_iota(jnp.int32, (TILE, ROWS), 1)
                scores[i] = jnp.where(col <= row, scores[i], NEG)
        return tuple(weigh(s, values, *c) for s, c in zip(scores, carry))

    start = ((jnp.full((TILE, 1), NEG, F32), jnp.zeros((TILE, HEAD), F32)),) * (2 * TILES)
    carry = lax.fori_loop(0, z, lambda i, c: update(i, c, tiles, False), start)
    lane = lax.broadcasted_iota(jnp.int32, (ROWS, HEAD), 1)
    for n, (turn, ref) in enumerate(zip(turns, (out0_ref, out1_ref))):
        mine = slice(n * TILES, (n + 1) * TILES)
        if turn == 0:
            last = update(z, carry[mine], tiles[mine], True)
        else:
            last = lax.cond(
                lax.rem(x + turn, NX) > x,
                lambda c, some=tiles[mine]: update(z, c, some, False),
                lambda c: c,
                carry[mine],
            )
        acc = jnp.concatenate([c[1] for c in last], axis=0)
        p_hi, p_mid, p_lo = three_pieces(jnp.concatenate([c[0] for c in last], axis=0))
        tail = jnp.where(
            lane == 0,
            p_hi.astype(F32),
            jnp.where(
                lane == 1,
                p_mid.astype(F32),
                jnp.where(lane == 2, p_lo.astype(F32), jnp.zeros((), F32)),
            ),
        )
        ref[...] = jnp.concatenate([acc, tail], axis=1).astype(BF16)


def combine_body(ids, gain_ref, *refs):
    out_ref, parts = refs[-1], refs[:-1]
    peaks = []
    for ref in parts:
        tail = ref[:, HEAD : HEAD + 3].astype(F32)
        peaks.append(tail[:, 0:1] + tail[:, 1:2] + tail[:, 2:3])
    top = jnp.maximum(jnp.maximum(peaks[0], peaks[1]), jnp.maximum(peaks[2], peaks[3]))
    total = jnp.zeros((ROWS, HEAD), F32)
    for ref, peak in zip(parts, peaks):
        total = total + ref[:, 0:HEAD].astype(F32) * jnp.exp2(peak - top)
    mean_square = jnp.mean(total * total, axis=1, keepdims=True)
    out = total * lax.rsqrt(mean_square + NORM_EPSILON) * gain_ref[...]
    out_ref[...] = out.T.astype(BF16)


def dispatch_body(ids, x_ref, gain_ref, routes_ref, table_ref, normed_ref, send_ref):
    c = ids[2]
    x = x_ref[...].astype(F32)
    mean_square = jnp.mean(x * x, axis=1, keepdims=True)
    normed = (x * lax.rsqrt(mean_square + NORM_EPSILON) * gain_ref[...]).astype(BF16)
    normed_ref[...] = normed
    expert = table_ref[:, 0:1] + 2 * c
    member = jnp.zeros((2 * SLOTS, TOK), F32)
    for k in range(4):
        member = jnp.where(routes_ref[k : k + 1, :] == expert, 1.0, member)
    before = lax.broadcasted_iota(jnp.int32, (TOK, TOK), 0)
    after = lax.broadcasted_iota(jnp.int32, (TOK, TOK), 1)
    earlier = jnp.where(before < after, 1.0, 0.0).astype(BF16)
    rank = dot(member.astype(BF16), earlier)
    pick = jnp.where(rank == table_ref[:, 1:2].astype(F32), member, 0.0)
    half = table_ref[:, 2:3]
    first = jnp.where(half == 0, pick, 0.0).astype(BF16)
    second = jnp.where(half == 1, pick, 0.0).astype(BF16)
    at = lax.rem(ids[3], 2) * (D // 2)
    low = normed_ref[:, pl.ds(pl.multiple_of(at, D // 2), D // 4)]
    high = normed_ref[:, pl.ds(pl.multiple_of(at + D // 4, D // 4), D // 4)]
    send_ref[...] = (dot(first, low) + dot(second, high)).astype(BF16)


def gated(g, u):
    return g / (1.0 + jnp.exp(-g)) * u


def experts_body(
    ids,
    x_ref,
    x_got_ref,
    gate_ref,
    up_ref,
    down_ref,
    got_ref,
    normed_ref,
    sgate_ref,
    sup_ref,
    sdown_ref,
    source_ref,
    out_ref,
    low_ref,
    high_ref,
):
    c = ids[2]
    even = lax.rem(ids[3], 2) == 0

    @pl.when(even)
    def _():
        low_ref[...] = x_ref[...]
        high_ref[...] = x_got_ref[...]

    @pl.when(jnp.logical_not(even))
    def _():
        low_ref[...] = x_got_ref[...]
        high_ref[...] = x_ref[...]

    lane = lax.broadcasted_iota(jnp.int32, (SLOTS, 2 * SLOTS), 1)
    x0 = jnp.where(lane == source_ref[:, 0:1], 1.0, 0.0).astype(BF16)
    x1 = jnp.where(lane == source_ref[:, 1:2], 1.0, 0.0).astype(BF16)
    low, high = low_ref[...], high_ref[...]
    rows = jnp.concatenate([dot(x0, low), dot(x1, low), dot(x0, high), dot(x1, high)], axis=1)
    rows = rows.astype(BF16)
    n = SLOTS // 2
    for l in range(LOCAL):
        wg = jnp.concatenate([gate_ref[l], got_ref[l * 64 : l * 64 + 64, :]], axis=0)
        wu = jnp.concatenate([up_ref[l], got_ref[128 + l * 64 : 128 + l * 64 + 64, :]], axis=0)
        g, u = dot_t(rows[l * n : (l + 1) * n], wg), dot_t(rows[l * n : (l + 1) * n], wu)
        h = gated(g, u).astype(BF16)
        wd = jnp.concatenate([down_ref[l], got_ref[256 + l * 64 : 320 + l * 64, :]], axis=0)
        part = dot(h, wd).astype(BF16)
        for to in range(NY * NC):
            out_ref[to, l * n : (l + 1) * n, :] = part[:, to * 128 : to * 128 + 128]
    tokens = normed_ref[pl.ds(pl.multiple_of(c * 64, 64), 64), :]
    wg = jnp.concatenate([sgate_ref[...], got_ref[384:416, :]], axis=0)
    wu = jnp.concatenate([sup_ref[...], got_ref[416:448, :]], axis=0)
    h = gated(dot_t(tokens, wg), dot_t(tokens, wu)).astype(BF16)
    wd = jnp.concatenate([sdown_ref[...], got_ref[448:480, :]], axis=0)
    part = dot(h, wd).astype(BF16)
    for to in range(NY * NC):
        out_ref[to, SLOTS : SLOTS + 64, :] = part[:, to * 128 : to * 128 + 128]


def sum_body(ids, part_ref, table_ref, out_ref, shared_ref):
    rows = []
    for c in range(NC):
        total = jnp.zeros((SLOTS + 64, 128), F32)
        for y in range(NY):
            total = total + part_ref[NC * y + c].astype(F32)
        shared_ref[c * 64 : c * 64 + 64, :] = total[SLOTS:]
        rows.append(total[:SLOTS].astype(BF16))
    lane = lax.broadcasted_iota(jnp.int32, (2 * SLOTS, SLOTS), 1)
    place = jnp.where(lane == table_ref[:, 3:4], 1.0, 0.0)
    half = table_ref[:, 2:3]
    first = jnp.where(half == 0, place, 0.0).astype(BF16)
    second = jnp.where(half == 1, place, 0.0).astype(BF16)
    out_ref[...] = (dot(first, rows[0]) + dot(second, rows[1])).astype(BF16)


def weigh_body(ids, y_ref, routes_ref, weight_ref, table_ref, shared_ref, out_ref):
    expert = table_ref[0:1, :] + 2 * table_ref[2:3, :]
    member = jnp.zeros((TOK, 2 * SLOTS), F32)
    weight = jnp.zeros((TOK, 2 * SLOTS), F32)
    for k in range(4):
        same = routes_ref[:, k : k + 1] == expert
        member = jnp.where(same, 1.0, member)
        weight = jnp.where(same, weight_ref[:, k : k + 1], weight)
    after = lax.broadcasted_iota(jnp.int32, (TOK, TOK), 0)
    before = lax.broadcasted_iota(jnp.int32, (TOK, TOK), 1)
    earlier = jnp.where(before < after, 1.0, 0.0).astype(BF16)
    rank = dot(earlier, member.astype(BF16))
    weight = jnp.where(rank == table_ref[1:2, :].astype(F32), weight, 0.0)
    total = shared_ref[...]
    for piece in three_pieces(weight):
        total = total + dot(piece, y_ref[...])
    out_ref[...] = total.astype(BF16)


def on_device(
    queries,
    keys,
    values,
    cum_gate,
    head_gain,
    moe_in,
    ffn_gain,
    routes,
    route_weight,
    expert_gate,
    expert_up,
    expert_down,
    shared_gate,
    shared_up,
    shared_down,
):
    z, x, y, c = (lax.axis_index(a) for a in ("z", "x", "y", "c"))
    ids = jnp.stack([z, x, c, y]).astype(jnp.int32)
    table = jnp.asarray(slot_table())
    source = jnp.asarray(source_table())
    swap = [(0, 1), (1, 0)]

    normed, sent = call(
        dispatch_body,
        (
            jax.ShapeDtypeStruct((TOK, D), BF16),
            jax.ShapeDtypeStruct((2 * SLOTS, D // 4), BF16),
        ),
        ids,
        (1,),
        [whole((TOK, D)), whole((1, D)), whole((4, TOK)), whole((2 * SLOTS, 8))],
        (whole((TOK, D)), whole((2 * SLOTS, D // 4))),
        (moe_in, ffn_gain.reshape(1, D), routes.T, table),
        flops=1_000_000_000,
    )
    arrived = lax.all_to_all(sent, ("z", "x"), 0, 0, tiled=True)
    arrived_too = lax.ppermute(arrived, "y", [(i, i ^ 1) for i in range(NY)])

    packed = call(
        pack_body,
        jax.ShapeDtypeStruct((KVG, ROWS), BF16),
        ids,
        (1,),
        [whole((HEAD, ROWS)), whole((HEAD, ROWS)), whole((1, ROWS)), UNREAD],
        whole((KVG, ROWS)),
        (keys.T, values.T, cum_gate.reshape(1, ROWS), sent),
    )
    rising, falling = [packed], [packed]
    for turn in range(1, 5):
        up = [(i, i + 1) for i in range(turn - 1, NZ - 1)]
        rising.append(lax.ppermute(rising[-1], "z", up))
        if turn < 4:
            down = [(i % NZ, (i - 1) % NZ) for i in range(1 - turn, 4 - turn)]
            falling.append(lax.ppermute(falling[-1], "z", down))
    kvg = rising + falling[:0:-1]

    other = pl.BlockSpec((LOCAL, 64, D), lambda i, s: (1 - s[2], 0, 0))
    trade = call(
        trade_body,
        jax.ShapeDtypeStruct((480, D), BF16),
        ids,
        (1,),
        [other, other, other, whole((32, D)), whole((32, D)), whole((32, D)), UNREAD],
        whole((480, D)),
        (expert_gate, expert_up, expert_down, shared_gate, shared_up, shared_down, sent),
        flops=1_000_000_000,
    )
    got = lax.ppermute(trade, "c", swap)

    mine, _ = lax.optimization_barrier((queries.T, trade))
    q_all = [mine]
    for d in range(1, NX):
        q_all.append(lax.ppermute(mine, "x", [((i + d) % NX, i) for i in range(NX)]))

    mine = pl.BlockSpec((LOCAL, 64, D), lambda i, s: (s[2], 0, 0))
    products = call(
        experts_body,
        jax.ShapeDtypeStruct((NY * NC, SLOTS + 64, 128), BF16),
        ids,
        (1,),
        [
            whole((2 * SLOTS, D // 4)),
            whole((2 * SLOTS, D // 4)),
            mine,
            mine,
            mine,
            whole((480, D)),
            whole((TOK, D)),
            whole((32, D)),
            whole((32, D)),
            whole((32, D)),
            whole((SLOTS, 8)),
        ],
        whole((NY * NC, SLOTS + 64, 128)),
        (
            arrived,
            arrived_too,
            expert_gate,
            expert_up,
            expert_down,
            got,
            normed,
            shared_gate,
            shared_up,
            shared_down,
            source,
        ),
        scratch=[pltpu.VMEM((2 * SLOTS, D // 4), BF16)] * 2,
        flops=1_000_000_000,
    )
    products = lax.all_to_all(products, ("y", "c"), 0, 0, tiled=True)

    def attend(turns):
        return call(
            functools.partial(attend_body, turns),
            (jax.ShapeDtypeStruct((ROWS, 128), BF16),) * 2,
            ids,
            (1,),
            [whole((HEAD, ROWS))] * 2 + [whole((KVG, ROWS))] * NZ,
            (whole((ROWS, 128)),) * 2,
            (q_all[turns[0]], q_all[turns[1]], *kvg),
            scratch=[pltpu.VMEM((NZ, DEPTH, ROWS), BF16), pltpu.VMEM((NZ, HEAD, ROWS), BF16)],
            flops=10_000_000_000,
        )

    def send_part(part, d):
        return lax.ppermute(part, "x", [(i, (i + d) % NX) for i in range(NX)])

    part1, part2 = attend((1, 2))
    part1, part2 = send_part(part1, 1), send_part(part2, 2)

    part3, part0 = attend((3, 0))
    part3 = send_part(part3, 3)

    rows, shared = call(
        sum_body,
        (
            jax.ShapeDtypeStruct((2 * SLOTS, 128), BF16),
            jax.ShapeDtypeStruct((TOK, 128), F32),
        ),
        ids,
        (1,),
        [whole((NY * NC, SLOTS + 64, 128)), whole((2 * SLOTS, 8))],
        (whole((2 * SLOTS, 128)), whole((TOK, 128))),
        (products, table),
        flops=1_000_000_000,
    )
    returned = lax.all_to_all(rows, ("z", "x"), 0, 0, tiled=True)

    mixed = call(
        combine_body,
        jax.ShapeDtypeStruct((HEAD, ROWS), BF16),
        ids,
        (1,),
        [whole((1, HEAD))] + [whole((ROWS, 128))] * NX,
        whole((HEAD, ROWS)),
        (head_gain.reshape(1, HEAD), part0, part1, part2, part3),
    ).T

    expert_out = call(
        weigh_body,
        jax.ShapeDtypeStruct((TOK, 128), BF16),
        ids,
        (1,),
        [
            whole((2 * SLOTS, 128)),
            whole((TOK, 4)),
            whole((TOK, 4)),
            whole((8, 2 * SLOTS)),
            whole((TOK, 128)),
        ],
        whole((TOK, 128)),
        (returned, routes, route_weight, table.T, shared),
        flops=1_000_000_000,
    )
    return (mixed, expert_out)


def solution(mesh):
    fine = Mesh(mesh.devices.reshape(NZ, NX, NY, NC), ("z", "x", "y", "c"))
    ep, tp = ("z", "x"), ("y", "c")
    in_specs = (
        P(ep, tp),
        P(ep, tp),
        P(ep, tp),
        P(ep, tp),
        P(tp),
        P(ep, None),
        P(),
        P(ep, None),
        P(ep, None),
        P(ep, tp, None),
        P(ep, tp, None),
        P(ep, tp, None),
        P(tp, None),
        P(tp, None),
        P(tp, None),
    )
    out_specs = (P(ep, tp), P(ep, tp))

    return jax.shard_map(
        on_device, mesh=fine, in_specs=in_specs, out_specs=out_specs, check_vma=False
    )
```

```python
import jax
import jax.numpy as jnp
import numpy as np
from jax import lax
from jax.experimental import pallas as pl
from jax.experimental.pallas import tpu as pltpu
from jax.sharding import Mesh
from jax.sharding import PartitionSpec as P


NORM_EPSILON = 1e-06
LOG2E = 1.4426950408889634
NEG = -1e30
NZ, NX, NY, NC = 8, 4, 8, 2
N_EP = NZ * NX
ROWS = 768
HEAD = 64
D = 2048
TOK = 128
CAP = 6
LOCAL = 2
SLOTS = N_EP * LOCAL * CAP
KG = HEAD + 16
KVG = KG + HEAD
F32 = jnp.float32
BF16 = jnp.bfloat16


def wide_slots():
    s = np.arange(2 * SLOTS)
    e, h, j = s // 24, (s % 24) // 12, s % 12
    return e, h, j // CAP, j % CAP


def slot_table():
    e, h, l, p = wide_slots()
    table = np.zeros((2 * SLOTS, 8), np.int32)
    table[:, 0] = 4 * e + l
    table[:, 1] = p
    table[:, 2] = h
    table[:, 3] = l * (SLOTS // 2) + e * CAP + p
    return table


def source_table():
    r = np.arange(SLOTS)
    l, e, p = r // (SLOTS // 2), (r % (SLOTS // 2)) // CAP, r % CAP
    table = np.zeros((SLOTS, 8), np.int32)
    table[:, 0] = e * 24 + l * CAP + p
    table[:, 1] = table[:, 0] + 12
    return table


def dot(a, b):
    return jnp.dot(a, b, preferred_element_type=F32)


def dot_t(a, b):
    return lax.dot_general(a, b, (((1,), (1,)), ((), ())), preferred_element_type=F32)


def three_pieces(v):
    hi = v.astype(BF16)
    rest = v - hi.astype(F32)
    mid = rest.astype(BF16)
    lo = (rest - mid.astype(F32)).astype(BF16)
    return hi, mid, lo


def call(body, out_shape, scalars, grid, in_specs, out_specs, args, scratch=(), flops=0, aliases=None):
    return pl.pallas_call(
        body,
        out_shape=out_shape,
        grid_spec=pltpu.PrefetchScalarGridSpec(
            num_scalar_prefetch=1,
            grid=grid,
            in_specs=in_specs,
            out_specs=out_specs,
            scratch_shapes=list(scratch),
        ),
        compiler_params=pltpu.CompilerParams(
            dimension_semantics=("arbitrary",) * len(grid), vmem_limit_bytes=56 * 2**20
        ),
        input_output_aliases=aliases or {},
        cost_estimate=pl.CostEstimate(flops=flops, bytes_accessed=4 << 20, transcendentals=0),
    )(scalars, *args)


def whole(shape):
    return pl.BlockSpec(shape, lambda i, s: (0,) * len(shape))


UNREAD = pl.BlockSpec(memory_space=pl.ANY)


def pack_body(ids, k_ref, v_ref, g_ref, after_ref, out_ref):
    out_ref[0:HEAD, :] = k_ref[...]
    out_ref[KG:KVG, :] = v_ref[...]
    hi, mid, lo = three_pieces(g_ref[...] * (-LOG2E))
    row = lax.broadcasted_iota(jnp.int32, (16, ROWS), 0)
    zero = jnp.zeros((16, ROWS), F32)
    pieces = jnp.where(
        row == 0,
        hi.astype(F32),
        jnp.where(row == 1, mid.astype(F32), jnp.where(row == 2, lo.astype(F32), zero)),
    )
    out_ref[HEAD:KG, :] = pieces.astype(BF16)


def trade_body(ids, gate_ref, up_ref, down_ref, sgate_ref, sup_ref, sdown_ref, after_ref, out_ref):
    for i, ref in enumerate((gate_ref, up_ref, down_ref)):
        for l in range(LOCAL):
            out_ref[i * 128 + l * 64 : i * 128 + l * 64 + 64, :] = ref[l]
    for i, ref in enumerate((sgate_ref, sup_ref, sdown_ref)):
        out_ref[384 + i * 32 : 416 + i * 32, :] = ref[...]


TILE = 384
TILES = ROWS // TILE
DEPTH = 2 * HEAD + 16


def attend_body(ids, *refs):
    queries, chunks, outs = refs[:NX], refs[NX : NX + NZ], refs[NX + NZ : -2]
    ka_ref, v_ref = refs[-2:]
    z, x = ids[0], ids[1]
    for back, ref in enumerate(chunks):
        place = lax.rem(z + NZ - back, NZ)
        ka_ref[place, 0:HEAD, :] = ref[0:HEAD, :]
        ka_ref[place, HEAD:DEPTH, :] = ref[0:KG, :]
        v_ref[place] = ref[KG:KVG, :]
    tiles = []
    for ref in queries:
        scaled = ref[...].astype(F32).T * (0.125 * LOG2E)
        hi = scaled.astype(BF16)
        lo = (scaled - hi.astype(F32)).astype(BF16)
        rows = jnp.concatenate([hi, lo, jnp.ones((ROWS, 16), BF16)], axis=1)
        tiles += [rows[i * TILE : (i + 1) * TILE] for i in range(TILES)]

    def weigh(s, values, peak, acc):
        new_peak = jnp.maximum(peak, jnp.max(s, axis=1, keepdims=True))
        w = jnp.exp2(s - new_peak).astype(BF16)
        return new_peak, acc * jnp.exp2(peak - new_peak) + dot_t(w, values)

    def update(chunk, carry, some, masked):
        k, values = ka_ref[chunk], v_ref[chunk]
        scores = [dot(tile, k) for tile in some]
        if masked:
            for i in range(TILES):
                row = lax.broadcasted_iota(jnp.int32, (TILE, ROWS), 0) + i * TILE
                col = lax.broadcasted_iota(jnp.int32, (TILE, ROWS), 1)
                scores[i] = jnp.where(col <= row, scores[i], NEG)
        return tuple(weigh(s, values, *c) for s, c in zip(scores, carry))

    start = ((jnp.full((TILE, 1), NEG, F32), jnp.zeros((TILE, HEAD), F32)),) * (NX * TILES)
    carry = lax.fori_loop(0, z, lambda i, c: update(i, c, tiles, False), start)
    lane = lax.broadcasted_iota(jnp.int32, (ROWS, HEAD), 1)
    for turn, ref in enumerate(outs):
        mine = slice(turn * TILES, (turn + 1) * TILES)
        if turn == 0:
            last = update(z, carry[mine], tiles[mine], True)
        else:
            last = lax.cond(
                lax.rem(x + turn, NX) > x,
                lambda c, some=tiles[mine]: update(z, c, some, False),
                lambda c: c,
                carry[mine],
            )
        acc = jnp.concatenate([c[1] for c in last], axis=0)
        p_hi, p_mid, p_lo = three_pieces(jnp.concatenate([c[0] for c in last], axis=0))
        tail = jnp.where(
            lane == 0,
            p_hi.astype(F32),
            jnp.where(
                lane == 1,
                p_mid.astype(F32),
                jnp.where(lane == 2, p_lo.astype(F32), jnp.zeros((), F32)),
            ),
        )
        ref[...] = jnp.concatenate([acc, tail], axis=1).astype(BF16)


def combine_body(ids, gain_ref, *refs):
    out_ref, parts = refs[-1], refs[:-1]
    peaks = []
    for ref in parts:
        tail = ref[:, HEAD : HEAD + 3].astype(F32)
        peaks.append(tail[:, 0:1] + tail[:, 1:2] + tail[:, 2:3])
    top = jnp.maximum(jnp.maximum(peaks[0], peaks[1]), jnp.maximum(peaks[2], peaks[3]))
    total = jnp.zeros((ROWS, HEAD), F32)
    for ref, peak in zip(parts, peaks):
        total = total + ref[:, 0:HEAD].astype(F32) * jnp.exp2(peak - top)
    mean_square = jnp.mean(total * total, axis=1, keepdims=True)
    out = total * lax.rsqrt(mean_square + NORM_EPSILON) * gain_ref[...]
    out_ref[...] = out.T.astype(BF16)


def dispatch_body(ids, x_ref, gain_ref, routes_ref, table_ref, normed_ref, send_ref):
    c = ids[2]
    x = x_ref[...].astype(F32)
    mean_square = jnp.mean(x * x, axis=1, keepdims=True)
    normed = (x * lax.rsqrt(mean_square + NORM_EPSILON) * gain_ref[...]).astype(BF16)
    normed_ref[...] = normed
    expert = table_ref[:, 0:1] + 2 * c
    member = jnp.zeros((2 * SLOTS, TOK), F32)
    for k in range(4):
        member = jnp.where(routes_ref[k : k + 1, :] == expert, 1.0, member)
    before = lax.broadcasted_iota(jnp.int32, (TOK, TOK), 0)
    after = lax.broadcasted_iota(jnp.int32, (TOK, TOK), 1)
    earlier = jnp.where(before < after, 1.0, 0.0).astype(BF16)
    rank = dot(member.astype(BF16), earlier)
    pick = jnp.where(rank == table_ref[:, 1:2].astype(F32), member, 0.0)
    half = table_ref[:, 2:3]
    first = jnp.where(half == 0, pick, 0.0).astype(BF16)
    second = jnp.where(half == 1, pick, 0.0).astype(BF16)
    at = lax.rem(ids[3], 2) * (D // 2)
    low = normed_ref[:, pl.ds(pl.multiple_of(at, D // 2), D // 4)]
    high = normed_ref[:, pl.ds(pl.multiple_of(at + D // 4, D // 4), D // 4)]
    send_ref[...] = (dot(first, low) + dot(second, high)).astype(BF16)


def gated(g, u):
    return g / (1.0 + jnp.exp(-g)) * u


def experts_body(
    ids,
    x_ref,
    x_got_ref,
    gate_ref,
    up_ref,
    down_ref,
    got_ref,
    normed_ref,
    sgate_ref,
    sup_ref,
    sdown_ref,
    source_ref,
    out_ref,
    low_ref,
    high_ref,
):
    c = ids[2]
    even = lax.rem(ids[3], 2) == 0

    @pl.when(even)
    def _():
        low_ref[...] = x_ref[...]
        high_ref[...] = x_got_ref[...]

    @pl.when(jnp.logical_not(even))
    def _():
        low_ref[...] = x_got_ref[...]
        high_ref[...] = x_ref[...]

    lane = lax.broadcasted_iota(jnp.int32, (SLOTS, 2 * SLOTS), 1)
    x0 = jnp.where(lane == source_ref[:, 0:1], 1.0, 0.0).astype(BF16)
    x1 = jnp.where(lane == source_ref[:, 1:2], 1.0, 0.0).astype(BF16)
    low, high = low_ref[...], high_ref[...]
    rows = jnp.concatenate([dot(x0, low), dot(x1, low), dot(x0, high), dot(x1, high)], axis=1)
    rows = rows.astype(BF16)
    n = SLOTS // 2
    for l in range(LOCAL):
        wg = jnp.concatenate([gate_ref[l], got_ref[l * 64 : l * 64 + 64, :]], axis=0)
        wu = jnp.concatenate([up_ref[l], got_ref[128 + l * 64 : 128 + l * 64 + 64, :]], axis=0)
        g, u = dot_t(rows[l * n : (l + 1) * n], wg), dot_t(rows[l * n : (l + 1) * n], wu)
        h = gated(g, u).astype(BF16)
        wd = jnp.concatenate([down_ref[l], got_ref[256 + l * 64 : 320 + l * 64, :]], axis=0)
        part = dot(h, wd).astype(BF16)
        for to in range(NY * NC):
            out_ref[to, l * n : (l + 1) * n, :] = part[:, to * 128 : to * 128 + 128]
    tokens = normed_ref[pl.ds(pl.multiple_of(c * 64, 64), 64), :]
    wg = jnp.concatenate([sgate_ref[...], got_ref[384:416, :]], axis=0)
    wu = jnp.concatenate([sup_ref[...], got_ref[416:448, :]], axis=0)
    h = gated(dot_t(tokens, wg), dot_t(tokens, wu)).astype(BF16)
    wd = jnp.concatenate([sdown_ref[...], got_ref[448:480, :]], axis=0)
    part = dot(h, wd).astype(BF16)
    for to in range(NY * NC):
        out_ref[to, SLOTS : SLOTS + 64, :] = part[:, to * 128 : to * 128 + 128]


def sum_body(ids, part_ref, table_ref, out_ref, shared_ref):
    rows = []
    for c in range(NC):
        total = jnp.zeros((SLOTS + 64, 128), F32)
        for y in range(NY):
            total = total + part_ref[NC * y + c].astype(F32)
        shared_ref[c * 64 : c * 64 + 64, :] = total[SLOTS:]
        rows.append(total[:SLOTS].astype(BF16))
    lane = lax.broadcasted_iota(jnp.int32, (2 * SLOTS, SLOTS), 1)
    place = jnp.where(lane == table_ref[:, 3:4], 1.0, 0.0)
    half = table_ref[:, 2:3]
    first = jnp.where(half == 0, place, 0.0).astype(BF16)
    second = jnp.where(half == 1, place, 0.0).astype(BF16)
    out_ref[...] = (dot(first, rows[0]) + dot(second, rows[1])).astype(BF16)


def weigh_body(ids, y_ref, routes_ref, weight_ref, table_ref, shared_ref, out_ref):
    expert = table_ref[0:1, :] + 2 * table_ref[2:3, :]
    member = jnp.zeros((TOK, 2 * SLOTS), F32)
    weight = jnp.zeros((TOK, 2 * SLOTS), F32)
    for k in range(4):
        same = routes_ref[:, k : k + 1] == expert
        member = jnp.where(same, 1.0, member)
        weight = jnp.where(same, weight_ref[:, k : k + 1], weight)
    after = lax.broadcasted_iota(jnp.int32, (TOK, TOK), 0)
    before = lax.broadcasted_iota(jnp.int32, (TOK, TOK), 1)
    earlier = jnp.where(before < after, 1.0, 0.0).astype(BF16)
    rank = dot(earlier, member.astype(BF16))
    weight = jnp.where(rank == table_ref[1:2, :].astype(F32), weight, 0.0)
    total = shared_ref[...]
    for piece in three_pieces(weight):
        total = total + dot(piece, y_ref[...])
    out_ref[...] = total.astype(BF16)


def on_device(
    queries,
    keys,
    values,
    cum_gate,
    head_gain,
    moe_in,
    ffn_gain,
    routes,
    route_weight,
    expert_gate,
    expert_up,
    expert_down,
    shared_gate,
    shared_up,
    shared_down,
):
    z, x, y, c = (lax.axis_index(a) for a in ("z", "x", "y", "c"))
    ids = jnp.stack([z, x, c, y]).astype(jnp.int32)
    table = jnp.asarray(slot_table())
    source = jnp.asarray(source_table())
    swap = [(0, 1), (1, 0)]

    normed, sent = call(
        dispatch_body,
        (
            jax.ShapeDtypeStruct((TOK, D), BF16),
            jax.ShapeDtypeStruct((2 * SLOTS, D // 4), BF16),
        ),
        ids,
        (1,),
        [whole((TOK, D)), whole((1, D)), whole((4, TOK)), whole((2 * SLOTS, 8))],
        (whole((TOK, D)), whole((2 * SLOTS, D // 4))),
        (moe_in, ffn_gain.reshape(1, D), routes.T, table),
        flops=1_000_000_000,
    )
    arrived = lax.all_to_all(sent, ("z", "x"), 0, 0, tiled=True)
    arrived_too = lax.ppermute(arrived, "y", [(i, i ^ 1) for i in range(NY)])

    packed = call(
        pack_body,
        jax.ShapeDtypeStruct((KVG, ROWS), BF16),
        ids,
        (1,),
        [whole((HEAD, ROWS)), whole((HEAD, ROWS)), whole((1, ROWS)), UNREAD],
        whole((KVG, ROWS)),
        (keys.T, values.T, cum_gate.reshape(1, ROWS), sent),
    )
    rising, falling = [packed], [packed]
    for turn in range(1, 5):
        up = [(i, i + 1) for i in range(turn - 1, NZ - 1)]
        rising.append(lax.ppermute(rising[-1], "z", up))
        if turn < 4:
            down = [(i % NZ, (i - 1) % NZ) for i in range(1 - turn, 4 - turn)]
            falling.append(lax.ppermute(falling[-1], "z", down))
    kvg = rising + falling[:0:-1]

    other = pl.BlockSpec((LOCAL, 64, D), lambda i, s: (1 - s[2], 0, 0))
    trade = call(
        trade_body,
        jax.ShapeDtypeStruct((480, D), BF16),
        ids,
        (1,),
        [other, other, other, whole((32, D)), whole((32, D)), whole((32, D)), UNREAD],
        whole((480, D)),
        (expert_gate, expert_up, expert_down, shared_gate, shared_up, shared_down, sent),
        flops=1_000_000_000,
    )
    got = lax.ppermute(trade, "c", swap)

    mine, _ = lax.optimization_barrier((queries.T, trade))
    q_all = [mine]
    for d in range(1, NX):
        q_all.append(lax.ppermute(mine, "x", [((i + d) % NX, i) for i in range(NX)]))

    mine = pl.BlockSpec((LOCAL, 64, D), lambda i, s: (s[2], 0, 0))
    products = call(
        experts_body,
        jax.ShapeDtypeStruct((NY * NC, SLOTS + 64, 128), BF16),
        ids,
        (1,),
        [
            whole((2 * SLOTS, D // 4)),
            whole((2 * SLOTS, D // 4)),
            mine,
            mine,
            mine,
            whole((480, D)),
            whole((TOK, D)),
            whole((32, D)),
            whole((32, D)),
            whole((32, D)),
            whole((SLOTS, 8)),
        ],
        whole((NY * NC, SLOTS + 64, 128)),
        (
            arrived,
            arrived_too,
            expert_gate,
            expert_up,
            expert_down,
            got,
            normed,
            shared_gate,
            shared_up,
            shared_down,
            source,
        ),
        scratch=[pltpu.VMEM((2 * SLOTS, D // 4), BF16)] * 2,
        flops=1_000_000_000,
    )
    products = lax.all_to_all(products, ("y", "c"), 0, 0, tiled=True)

    parts = call(
        attend_body,
        (jax.ShapeDtypeStruct((ROWS, 128), BF16),) * NX,
        ids,
        (1,),
        [whole((HEAD, ROWS))] * NX + [whole((KVG, ROWS))] * NZ,
        (whole((ROWS, 128)),) * NX,
        (*q_all, *kvg),
        scratch=[pltpu.VMEM((NZ, DEPTH, ROWS), BF16), pltpu.VMEM((NZ, HEAD, ROWS), BF16)],
        flops=20_000_000_000,
    )
    parts = [parts[0]] + [
        lax.ppermute(parts[d], "x", [(i, (i + d) % NX) for i in range(NX)])
        for d in range(1, NX)
    ]

    rows, shared = call(
        sum_body,
        (
            jax.ShapeDtypeStruct((2 * SLOTS, 128), BF16),
            jax.ShapeDtypeStruct((TOK, 128), F32),
        ),
        ids,
        (1,),
        [whole((NY * NC, SLOTS + 64, 128)), whole((2 * SLOTS, 8))],
        (whole((2 * SLOTS, 128)), whole((TOK, 128))),
        (products, table),
        flops=1_000_000_000,
    )
    returned = lax.all_to_all(rows, ("z", "x"), 0, 0, tiled=True)

    mixed = call(
        combine_body,
        jax.ShapeDtypeStruct((HEAD, ROWS), BF16),
        ids,
        (1,),
        [whole((1, HEAD))] + [whole((ROWS, 128))] * NX,
        whole((HEAD, ROWS)),
        (head_gain.reshape(1, HEAD), *parts),
    ).T

    expert_out = call(
        weigh_body,
        jax.ShapeDtypeStruct((TOK, 128), BF16),
        ids,
        (1,),
        [
            whole((2 * SLOTS, 128)),
            whole((TOK, 4)),
            whole((TOK, 4)),
            whole((8, 2 * SLOTS)),
            whole((TOK, 128)),
        ],
        whole((TOK, 128)),
        (returned, routes, route_weight, table.T, shared),
        flops=1_000_000_000,
    )
    return (mixed, expert_out)


def solution(mesh):
    fine = Mesh(mesh.devices.reshape(NZ, NX, NY, NC), ("z", "x", "y", "c"))
    ep, tp = ("z", "x"), ("y", "c")
    in_specs = (
        P(ep, tp),
        P(ep, tp),
        P(ep, tp),
        P(ep, tp),
        P(tp),
        P(ep, None),
        P(),
        P(ep, None),
        P(ep, None),
        P(ep, tp, None),
        P(ep, tp, None),
        P(ep, tp, None),
        P(tp, None),
        P(tp, None),
        P(tp, None),
    )
    out_specs = (P(ep, tp), P(ep, tp))

    return jax.shard_map(
        on_device, mesh=fine, in_specs=in_specs, out_specs=out_specs, check_vma=False
    )
```

```python
import jax
import jax.numpy as jnp
import numpy as np
from jax import lax
from jax.experimental import pallas as pl
from jax.experimental.pallas import tpu as pltpu
from jax.sharding import Mesh
from jax.sharding import PartitionSpec as P


NORM_EPSILON = 1e-06
LOG2E = 1.4426950408889634
NEG = -1e30
NZ, NX, NY, NC = 8, 4, 8, 2
N_EP = NZ * NX
ROWS = 768
HEAD = 64
D = 2048
TOK = 128
CAP = 6
LOCAL = 2
SLOTS = N_EP * LOCAL * CAP
KG = HEAD + 16
KVG = KG + HEAD
F32 = jnp.float32
BF16 = jnp.bfloat16


def wide_slots():
    s = np.arange(2 * SLOTS)
    e, h, j = s // 24, (s % 24) // 12, s % 12
    return e, h, j // CAP, j % CAP


def slot_table():
    e, h, l, p = wide_slots()
    table = np.zeros((2 * SLOTS, 8), np.int32)
    table[:, 0] = 4 * e + l
    table[:, 1] = p
    table[:, 2] = h
    table[:, 3] = l * (SLOTS // 2) + e * CAP + p
    return table


def source_table():
    r = np.arange(SLOTS)
    l, e, p = r // (SLOTS // 2), (r % (SLOTS // 2)) // CAP, r % CAP
    table = np.zeros((SLOTS, 8), np.int32)
    table[:, 0] = e * 24 + l * CAP + p
    table[:, 1] = table[:, 0] + 12
    return table


def dot(a, b):
    return jnp.dot(a, b, preferred_element_type=F32)


def dot_t(a, b):
    return lax.dot_general(a, b, (((1,), (1,)), ((), ())), preferred_element_type=F32)


def three_pieces(v):
    hi = v.astype(BF16)
    rest = v - hi.astype(F32)
    mid = rest.astype(BF16)
    lo = (rest - mid.astype(F32)).astype(BF16)
    return hi, mid, lo


def call(body, out_shape, scalars, grid, in_specs, out_specs, args, scratch=(), flops=0, aliases=None):
    return pl.pallas_call(
        body,
        out_shape=out_shape,
        grid_spec=pltpu.PrefetchScalarGridSpec(
            num_scalar_prefetch=1,
            grid=grid,
            in_specs=in_specs,
            out_specs=out_specs,
            scratch_shapes=list(scratch),
        ),
        compiler_params=pltpu.CompilerParams(
            dimension_semantics=("arbitrary",) * len(grid), vmem_limit_bytes=56 * 2**20
        ),
        input_output_aliases=aliases or {},
        cost_estimate=pl.CostEstimate(flops=flops, bytes_accessed=4 << 20, transcendentals=0),
    )(scalars, *args)


def whole(shape):
    return pl.BlockSpec(shape, lambda i, s: (0,) * len(shape))


UNREAD = pl.BlockSpec(memory_space=pl.ANY)


def pack_body(ids, k_ref, v_ref, g_ref, after_ref, out_ref):
    out_ref[0:HEAD, :] = k_ref[...]
    out_ref[KG:KVG, :] = v_ref[...]
    hi, mid, lo = three_pieces(g_ref[...] * (-LOG2E))
    row = lax.broadcasted_iota(jnp.int32, (16, ROWS), 0)
    zero = jnp.zeros((16, ROWS), F32)
    pieces = jnp.where(
        row == 0,
        hi.astype(F32),
        jnp.where(row == 1, mid.astype(F32), jnp.where(row == 2, lo.astype(F32), zero)),
    )
    out_ref[HEAD:KG, :] = pieces.astype(BF16)


def trade_body(ids, gate_ref, up_ref, down_ref, sgate_ref, sup_ref, sdown_ref, after_ref, out_ref):
    for i, ref in enumerate((gate_ref, up_ref, down_ref)):
        for l in range(LOCAL):
            out_ref[i * 128 + l * 64 : i * 128 + l * 64 + 64, :] = ref[l]
    for i, ref in enumerate((sgate_ref, sup_ref, sdown_ref)):
        out_ref[384 + i * 32 : 416 + i * 32, :] = ref[...]


TILE = 384
TILES = ROWS // TILE
DEPTH = 2 * HEAD + 16


def attend_body(ids, *refs):
    queries, chunks, outs = refs[:NX], refs[NX : NX + NZ], refs[NX + NZ : -2]
    ka_ref, v_ref = refs[-2:]
    z, x = ids[0], ids[1]
    for back, ref in enumerate(chunks):
        place = lax.rem(z + NZ - back, NZ)
        ka_ref[place, 0:HEAD, :] = ref[0:HEAD, :]
        ka_ref[place, HEAD:DEPTH, :] = ref[0:KG, :]
        v_ref[place] = ref[KG:KVG, :]
    tiles = []
    for ref in queries:
        scaled = ref[...].astype(F32).T * (0.125 * LOG2E)
        hi = scaled.astype(BF16)
        lo = (scaled - hi.astype(F32)).astype(BF16)
        rows = jnp.concatenate([hi, lo, jnp.ones((ROWS, 16), BF16)], axis=1)
        tiles += [rows[i * TILE : (i + 1) * TILE] for i in range(TILES)]

    def weigh(s, values, peak, acc):
        new_peak = jnp.maximum(peak, jnp.max(s, axis=1, keepdims=True))
        w = jnp.exp2(s - new_peak).astype(BF16)
        return new_peak, acc * jnp.exp2(peak - new_peak) + dot_t(w, values)

    def update(chunk, carry, some, masked):
        k, values = ka_ref[chunk], v_ref[chunk]
        scores = [dot(tile, k) for tile in some]
        if masked:
            for i in range(TILES):
                row = lax.broadcasted_iota(jnp.int32, (TILE, ROWS), 0) + i * TILE
                col = lax.broadcasted_iota(jnp.int32, (TILE, ROWS), 1)
                scores[i] = jnp.where(col <= row, scores[i], NEG)
        return tuple(weigh(s, values, *c) for s, c in zip(scores, carry))

    start = ((jnp.full((TILE, 1), NEG, F32), jnp.zeros((TILE, HEAD), F32)),) * (NX * TILES)
    carry = lax.fori_loop(0, z, lambda i, c: update(i, c, tiles, False), start)
    lane = lax.broadcasted_iota(jnp.int32, (ROWS, HEAD), 1)
    for turn, ref in enumerate(outs):
        mine = slice(turn * TILES, (turn + 1) * TILES)
        if turn == 0:
            last = update(z, carry[mine], tiles[mine], True)
        else:
            last = lax.cond(
                lax.rem(x + turn, NX) > x,
                lambda c, some=tiles[mine]: update(z, c, some, False),
                lambda c: c,
                carry[mine],
            )
        acc = jnp.concatenate([c[1] for c in last], axis=0)
        p_hi, p_mid, p_lo = three_pieces(jnp.concatenate([c[0] for c in last], axis=0))
        tail = jnp.where(
            lane == 0,
            p_hi.astype(F32),
            jnp.where(
                lane == 1,
                p_mid.astype(F32),
                jnp.where(lane == 2, p_lo.astype(F32), jnp.zeros((), F32)),
            ),
        )
        ref[...] = jnp.concatenate([acc, tail], axis=1).astype(BF16)


def combine_body(ids, gain_ref, *refs):
    out_ref, parts = refs[-1], refs[:-1]
    peaks = []
    for ref in parts:
        tail = ref[:, HEAD : HEAD + 3].astype(F32)
        peaks.append(tail[:, 0:1] + tail[:, 1:2] + tail[:, 2:3])
    top = jnp.maximum(jnp.maximum(peaks[0], peaks[1]), jnp.maximum(peaks[2], peaks[3]))
    total = jnp.zeros((ROWS, HEAD), F32)
    for ref, peak in zip(parts, peaks):
        total = total + ref[:, 0:HEAD].astype(F32) * jnp.exp2(peak - top)
    mean_square = jnp.mean(total * total, axis=1, keepdims=True)
    out = total * lax.rsqrt(mean_square + NORM_EPSILON) * gain_ref[...]
    out_ref[...] = out.T.astype(BF16)


def dispatch_body(ids, x_ref, gain_ref, routes_ref, table_ref, normed_ref, send_ref):
    c = ids[2]
    x = x_ref[...].astype(F32)
    mean_square = jnp.mean(x * x, axis=1, keepdims=True)
    normed = (x * lax.rsqrt(mean_square + NORM_EPSILON) * gain_ref[...]).astype(BF16)
    normed_ref[...] = normed
    expert = table_ref[:, 0:1] + 2 * c
    member = jnp.zeros((2 * SLOTS, TOK), F32)
    for k in range(4):
        member = jnp.where(routes_ref[k : k + 1, :] == expert, 1.0, member)
    before = lax.broadcasted_iota(jnp.int32, (TOK, TOK), 0)
    after = lax.broadcasted_iota(jnp.int32, (TOK, TOK), 1)
    earlier = jnp.where(before < after, 1.0, 0.0).astype(BF16)
    rank = dot(member.astype(BF16), earlier)
    pick = jnp.where(rank == table_ref[:, 1:2].astype(F32), member, 0.0)
    half = table_ref[:, 2:3]
    first = jnp.where(half == 0, pick, 0.0).astype(BF16)
    second = jnp.where(half == 1, pick, 0.0).astype(BF16)
    at = lax.rem(ids[3], 2) * (D // 2)
    low = normed_ref[:, pl.ds(pl.multiple_of(at, D // 2), D // 4)]
    high = normed_ref[:, pl.ds(pl.multiple_of(at + D // 4, D // 4), D // 4)]
    send_ref[...] = (dot(first, low) + dot(second, high)).astype(BF16)


def gated(g, u):
    return g / (1.0 + jnp.exp(-g)) * u


def experts_body(
    ids,
    x_ref,
    x_below_ref,
    x_above_ref,
    gate_ref,
    up_ref,
    down_ref,
    got_ref,
    normed_ref,
    sgate_ref,
    sup_ref,
    sdown_ref,
    source_ref,
    out_ref,
    low_ref,
    high_ref,
):
    c = ids[2]
    even = lax.rem(ids[3], 2) == 0

    @pl.when(even)
    def _():
        low_ref[...] = x_ref[...]
        high_ref[0:SLOTS, :] = x_below_ref[...]
        high_ref[SLOTS:, :] = x_above_ref[...]

    @pl.when(jnp.logical_not(even))
    def _():
        low_ref[0:SLOTS, :] = x_below_ref[...]
        low_ref[SLOTS:, :] = x_above_ref[...]
        high_ref[...] = x_ref[...]

    lane = lax.broadcasted_iota(jnp.int32, (SLOTS, 2 * SLOTS), 1)
    x0 = jnp.where(lane == source_ref[:, 0:1], 1.0, 0.0).astype(BF16)
    x1 = jnp.where(lane == source_ref[:, 1:2], 1.0, 0.0).astype(BF16)
    low, high = low_ref[...], high_ref[...]
    rows = jnp.concatenate([dot(x0, low), dot(x1, low), dot(x0, high), dot(x1, high)], axis=1)
    rows = rows.astype(BF16)
    n = SLOTS // 2
    for l in range(LOCAL):
        wg = jnp.concatenate([gate_ref[l], got_ref[l * 64 : l * 64 + 64, :]], axis=0)
        wu = jnp.concatenate([up_ref[l], got_ref[128 + l * 64 : 128 + l * 64 + 64, :]], axis=0)
        g, u = dot_t(rows[l * n : (l + 1) * n], wg), dot_t(rows[l * n : (l + 1) * n], wu)
        h = gated(g, u).astype(BF16)
        wd = jnp.concatenate([down_ref[l], got_ref[256 + l * 64 : 320 + l * 64, :]], axis=0)
        part = dot(h, wd).astype(BF16)
        for to in range(NY * NC):
            out_ref[to, l * n : (l + 1) * n, :] = part[:, to * 128 : to * 128 + 128]
    tokens = normed_ref[pl.ds(pl.multiple_of(c * 64, 64), 64), :]
    wg = jnp.concatenate([sgate_ref[...], got_ref[384:416, :]], axis=0)
    wu = jnp.concatenate([sup_ref[...], got_ref[416:448, :]], axis=0)
    h = gated(dot_t(tokens, wg), dot_t(tokens, wu)).astype(BF16)
    wd = jnp.concatenate([sdown_ref[...], got_ref[448:480, :]], axis=0)
    part = dot(h, wd).astype(BF16)
    for to in range(NY * NC):
        out_ref[to, SLOTS : SLOTS + 64, :] = part[:, to * 128 : to * 128 + 128]


def sum_body(ids, part_ref, table_ref, out_ref, shared_ref):
    rows = []
    for c in range(NC):
        total = jnp.zeros((SLOTS + 64, 128), F32)
        for y in range(NY):
            total = total + part_ref[NC * y + c].astype(F32)
        shared_ref[c * 64 : c * 64 + 64, :] = total[SLOTS:]
        rows.append(total[:SLOTS].astype(BF16))
    lane = lax.broadcasted_iota(jnp.int32, (2 * SLOTS, SLOTS), 1)
    place = jnp.where(lane == table_ref[:, 3:4], 1.0, 0.0)
    half = table_ref[:, 2:3]
    first = jnp.where(half == 0, place, 0.0).astype(BF16)
    second = jnp.where(half == 1, place, 0.0).astype(BF16)
    out_ref[...] = (dot(first, rows[0]) + dot(second, rows[1])).astype(BF16)


def weigh_body(ids, y_ref, routes_ref, weight_ref, table_ref, shared_ref, out_ref):
    expert = table_ref[0:1, :] + 2 * table_ref[2:3, :]
    member = jnp.zeros((TOK, 2 * SLOTS), F32)
    weight = jnp.zeros((TOK, 2 * SLOTS), F32)
    for k in range(4):
        same = routes_ref[:, k : k + 1] == expert
        member = jnp.where(same, 1.0, member)
        weight = jnp.where(same, weight_ref[:, k : k + 1], weight)
    after = lax.broadcasted_iota(jnp.int32, (TOK, TOK), 0)
    before = lax.broadcasted_iota(jnp.int32, (TOK, TOK), 1)
    earlier = jnp.where(before < after, 1.0, 0.0).astype(BF16)
    rank = dot(earlier, member.astype(BF16))
    weight = jnp.where(rank == table_ref[1:2, :].astype(F32), weight, 0.0)
    total = shared_ref[...]
    for piece in three_pieces(weight):
        total = total + dot(piece, y_ref[...])
    out_ref[...] = total.astype(BF16)


def on_device(
    queries,
    keys,
    values,
    cum_gate,
    head_gain,
    moe_in,
    ffn_gain,
    routes,
    route_weight,
    expert_gate,
    expert_up,
    expert_down,
    shared_gate,
    shared_up,
    shared_down,
):
    z, x, y, c = (lax.axis_index(a) for a in ("z", "x", "y", "c"))
    ids = jnp.stack([z, x, c, y]).astype(jnp.int32)
    table = jnp.asarray(slot_table())
    source = jnp.asarray(source_table())
    swap = [(0, 1), (1, 0)]

    normed, sent = call(
        dispatch_body,
        (
            jax.ShapeDtypeStruct((TOK, D), BF16),
            jax.ShapeDtypeStruct((2 * SLOTS, D // 4), BF16),
        ),
        ids,
        (1,),
        [whole((TOK, D)), whole((1, D)), whole((4, TOK)), whole((2 * SLOTS, 8))],
        (whole((TOK, D)), whole((2 * SLOTS, D // 4))),
        (moe_in, ffn_gain.reshape(1, D), routes.T, table),
        flops=1_000_000_000,
    )
    arrived = lax.all_to_all(sent, ("z", "x"), 0, 0, tiled=True)
    arrived_too = [
        lax.ppermute(arrived[:SLOTS], "y", [(i, (i + 1) % NY) for i in range(NY)]),
        lax.ppermute(arrived[SLOTS:], "y", [(i, (i - 1) % NY) for i in range(NY)]),
    ]

    packed = call(
        pack_body,
        jax.ShapeDtypeStruct((KVG, ROWS), BF16),
        ids,
        (1,),
        [whole((HEAD, ROWS)), whole((HEAD, ROWS)), whole((1, ROWS)), UNREAD],
        whole((KVG, ROWS)),
        (keys.T, values.T, cum_gate.reshape(1, ROWS), sent),
    )
    rising, falling = [packed], [packed]
    for turn in range(1, 5):
        up = [(i, i + 1) for i in range(turn - 1, NZ - 1)]
        rising.append(lax.ppermute(rising[-1], "z", up))
        if turn < 4:
            down = [(i % NZ, (i - 1) % NZ) for i in range(1 - turn, 4 - turn)]
            falling.append(lax.ppermute(falling[-1], "z", down))
    kvg = rising + falling[:0:-1]

    other = pl.BlockSpec((LOCAL, 64, D), lambda i, s: (1 - s[2], 0, 0))
    trade = call(
        trade_body,
        jax.ShapeDtypeStruct((480, D), BF16),
        ids,
        (1,),
        [other, other, other, whole((32, D)), whole((32, D)), whole((32, D)), UNREAD],
        whole((480, D)),
        (expert_gate, expert_up, expert_down, shared_gate, shared_up, shared_down, sent),
        flops=1_000_000_000,
    )
    got = lax.ppermute(trade, "c", swap)

    mine, _ = lax.optimization_barrier((queries.T, trade))
    q_all = [mine]
    for d in range(1, NX):
        q_all.append(lax.ppermute(mine, "x", [((i + d) % NX, i) for i in range(NX)]))

    mine = pl.BlockSpec((LOCAL, 64, D), lambda i, s: (s[2], 0, 0))
    products = call(
        experts_body,
        jax.ShapeDtypeStruct((NY * NC, SLOTS + 64, 128), BF16),
        ids,
        (1,),
        [
            whole((2 * SLOTS, D // 4)),
            whole((SLOTS, D // 4)),
            whole((SLOTS, D // 4)),
            mine,
            mine,
            mine,
            whole((480, D)),
            whole((TOK, D)),
            whole((32, D)),
            whole((32, D)),
            whole((32, D)),
            whole((SLOTS, 8)),
        ],
        whole((NY * NC, SLOTS + 64, 128)),
        (
            arrived,
            *arrived_too,
            expert_gate,
            expert_up,
            expert_down,
            got,
            normed,
            shared_gate,
            shared_up,
            shared_down,
            source,
        ),
        scratch=[pltpu.VMEM((2 * SLOTS, D // 4), BF16)] * 2,
        flops=1_000_000_000,
    )
    products = lax.all_to_all(products, ("y", "c"), 0, 0, tiled=True)

    parts = call(
        attend_body,
        (jax.ShapeDtypeStruct((ROWS, 128), BF16),) * NX,
        ids,
        (1,),
        [whole((HEAD, ROWS))] * NX + [whole((KVG, ROWS))] * NZ,
        (whole((ROWS, 128)),) * NX,
        (*q_all, *kvg),
        scratch=[pltpu.VMEM((NZ, DEPTH, ROWS), BF16), pltpu.VMEM((NZ, HEAD, ROWS), BF16)],
        flops=20_000_000_000,
    )
    parts = [parts[0]] + [
        lax.ppermute(parts[d], "x", [(i, (i + d) % NX) for i in range(NX)])
        for d in range(1, NX)
    ]

    rows, shared = call(
        sum_body,
        (
            jax.ShapeDtypeStruct((2 * SLOTS, 128), BF16),
            jax.ShapeDtypeStruct((TOK, 128), F32),
        ),
        ids,
        (1,),
        [whole((NY * NC, SLOTS + 64, 128)), whole((2 * SLOTS, 8))],
        (whole((2 * SLOTS, 128)), whole((TOK, 128))),
        (products, table),
        flops=1_000_000_000,
    )
    returned = lax.all_to_all(rows, ("z", "x"), 0, 0, tiled=True)

    mixed = call(
        combine_body,
        jax.ShapeDtypeStruct((HEAD, ROWS), BF16),
        ids,
        (1,),
        [whole((1, HEAD))] + [whole((ROWS, 128))] * NX,
        whole((HEAD, ROWS)),
        (head_gain.reshape(1, HEAD), *parts),
    ).T

    expert_out = call(
        weigh_body,
        jax.ShapeDtypeStruct((TOK, 128), BF16),
        ids,
        (1,),
        [
            whole((2 * SLOTS, 128)),
            whole((TOK, 4)),
            whole((TOK, 4)),
            whole((8, 2 * SLOTS)),
            whole((TOK, 128)),
        ],
        whole((TOK, 128)),
        (returned, routes, route_weight, table.T, shared),
        flops=1_000_000_000,
    )
    return (mixed, expert_out)


def solution(mesh):
    fine = Mesh(mesh.devices.reshape(NZ, NX, NY, NC), ("z", "x", "y", "c"))
    ep, tp = ("z", "x"), ("y", "c")
    in_specs = (
        P(ep, tp),
        P(ep, tp),
        P(ep, tp),
        P(ep, tp),
        P(tp),
        P(ep, None),
        P(),
        P(ep, None),
        P(ep, None),
        P(ep, tp, None),
        P(ep, tp, None),
        P(ep, tp, None),
        P(tp, None),
        P(tp, None),
        P(tp, None),
    )
    out_specs = (P(ep, tp), P(ep, tp))

    return jax.shard_map(
        on_device, mesh=fine, in_specs=in_specs, out_specs=out_specs, check_vma=False
    )
```
